32 devices in a mesh: sp: 16 (over z, y, x), tp: 2 (over core).
Axes of the slice: x: 2, y: 2, z: 4, core: 2. Of those that a mesh axis runs over, the one named last changes fastest.
Arguments:
- tokens: bfloat16 [4608, 4096], P('sp', 'tp'), may hold values from -6 to 6
- doc_ids: int32 [4608], P('sp'), may hold values from 0 to 3, never falling along the last dimension, each value on 1 to 2304 neighbouring positions
- norm_gain: float32 [2, 4096], replicated, may hold values from 0.1 to 1.9
- in_proj: bfloat16 [2, 4096, 4096], P(None, 'sp', 'tp'), may hold values from -0.09375 to 0.09375
- mix_proj: bfloat16 [2, 1024, 4096], P(None, 'sp', 'tp'), may hold values from -0.1875 to 0.1875
- out_scale: float32 [2, 4096], replicated, may hold values from 0.1 to 1.9
Outputs:
- mixed_out: bfloat16 [4608, 4096], P('sp', 'tp')
The draws below stay inside these ranges and needn't reach their ends.
Inputs may be any that keep to these rules, and one draw needn't show every extreme that they name: `doc_ids`: document numbers never fall along the sequence, run from 0 to 3, and each document holds at most 2304 positions.
All inputs are finite; a program needn't handle non-finite values.
Results may differ from the reference program's by a relative error of at most 0.0085.
Values may be sent and summed in bfloat16 or wider, within the bound.
A program may use at most 128 MiB of HBM per device.

```python
import math
import jax
import jax.numpy as jnp
import numpy as np
from jax import lax

D = 4096
GROUP = 1024
WIN = 16
LAYERS = 2
TOKENS = 4608
DOCS = 4


def block_levels(key, extent, shards, low, largest):
    gain, own = 1.0, jax.random.fold_in(key, 6)
    for dim, shards_of in shards:
        heights = jnp.exp(jax.random.uniform(jax.random.fold_in(own, dim), (shards_of,), jnp.float32, low / len(shards), largest / len(shards)))
        gain = gain * jnp.repeat(heights, extent[dim] // shards_of).reshape([-1 if axis == dim else 1 for axis in range(len(extent))])
    return gain


def length_profile(count, total, most, skew):
    weights = [(1 << 20) // math.isqrt(standing ** skew) + 1 for standing in range(2, count + 1)]
    rest, counts = total - most - (count - 1), [1] * (count - 1)
    while rest > 0:
        free = [i for i in range(count - 1) if counts[i] < most]
        whole, budget = sum([weights[i] for i in free]), rest
        for i in free:
            extra = min(most - counts[i], max(1, budget * weights[i] // whole), rest)
            counts[i] = counts[i] + extra
            rest = rest - extra
    return np.array([most] + counts)


def uneven(stream_key, amount, total, most, slope):
    if amount == 2:
        one = jax.random.randint(stream_key, (), max(1, total - most), min(most, total - 1) + 1)
        return jnp.stack([one, total - one])
    tallies = jnp.asarray(length_profile(amount, total, most, slope), jnp.int32)
    couples = (amount - 1) // 2
    source_of, taker = tallies[1:1 + 2 * couples:2], tallies[2:2 + 2 * couples:2]
    margin = jnp.minimum(source_of - 1, most - taker)
    moved = jax.random.randint(jax.random.fold_in(stream_key, 1), (couples,), 0, 1 << 20) % (margin + 1)
    tallies = tallies.at[1:1 + 2 * couples:2].set(source_of - moved).at[2:2 + 2 * couples:2].set(taker + moved)
    return tallies[jax.random.permutation(jax.random.fold_in(stream_key, 2), amount)]


def scatter_about(rng, dims, spread, limit, shards=(), kind=jnp.bfloat16):
    values = spread * jax.random.normal(rng, dims, jnp.float32)
    if shards:
        values = values * block_levels(rng, dims, shards, -0.22, 0.18)
    return jnp.clip(values, -limit, limit).astype(kind)


def setup_inputs(seed: int = 0) -> dict:
    splits = jax.random.split(jax.random.key(seed), 7)
    tokens = scatter_about(splits[0], (TOKENS, D), 1.0, 6.0, ((0, 16), (1, 2)))
    doc_ids = jnp.searchsorted(jnp.cumsum(uneven(splits[1], DOCS, TOKENS, TOKENS // 2, 1)), jnp.arange(TOKENS), side="right").astype(jnp.int32)
    norm_gain = jnp.clip(1.0 + 0.18 * jax.random.normal(splits[2], (LAYERS, D), jnp.float32), 0.1, 1.9)
    in_proj = scatter_about(splits[3], (LAYERS, D, D), D ** -0.5, 0.09375, ((1, 16), (2, 2)))
    mix_proj = scatter_about(splits[4], (LAYERS, GROUP, D), GROUP ** -0.5, 0.1875, ((1, 16), (2, 2)))
    out_scale = jnp.clip(1.0 + 0.18 * jax.random.normal(splits[5], (LAYERS, D), jnp.float32), 0.1, 1.9)
    return {"tokens": tokens, "doc_ids": doc_ids, "norm_gain": norm_gain, "in_proj": in_proj, "mix_proj": mix_proj, "out_scale": out_scale}


epsilon = 1e-06

def pool_all(proj_f32, doc_ids, windows):
    padded = jnp.concatenate([jnp.zeros((WIN - 1, D), jnp.float32), proj_f32], axis=0)
    padded_docs = jnp.concatenate([jnp.full((WIN - 1,), -1, jnp.int32), doc_ids.astype(jnp.int32)], axis=0)
    window_sum = jnp.zeros_like(proj_f32)
    window_count = jnp.zeros_like(proj_f32)
    for offset in range(WIN):
        begin = WIN - 1 - offset
        shifted = padded[begin:begin + TOKENS]
        same_doc = padded_docs[begin:begin + TOKENS] == doc_ids
        taken = same_doc[:, None] & (offset < windows)[None, :]
        window_sum = window_sum + jnp.where(taken, shifted, jnp.float32(0.0))
        window_count = window_count + taken.astype(jnp.float32)
    return (window_sum / window_count - proj_f32).astype(jnp.bfloat16)

def reference(tokens, doc_ids, norm_gain, in_proj, mix_proj, out_scale):
    block_width = D // 8
    channels = jnp.arange(D, dtype=jnp.int32)
    windows = jnp.left_shift(jnp.int32(2), channels // block_width % 4)
    current = tokens
    for depth_idx in range(LAYERS):
        values = current.astype(jnp.float32)
        scaled = values * lax.rsqrt(lax.optimization_barrier(jnp.mean(values * values, axis=-1, keepdims=True)) + epsilon)
        normed = (scaled * norm_gain[depth_idx][None, :]).astype(jnp.bfloat16)
        projected = jnp.dot(normed, in_proj[depth_idx], preferred_element_type=jnp.float32).astype(jnp.bfloat16)
        pooled = pool_all(projected.astype(jnp.float32), doc_ids, windows)
        blocks_out = [None] * 8
        for group_idx in range(4):
            first = group_idx * block_width
            second = (group_idx + 4) * block_width
            inputs = jnp.concatenate([pooled[:, first:first + block_width], pooled[:, second:second + block_width]], axis=1)
            weights = jnp.concatenate([mix_proj[depth_idx][:, first:first + block_width], mix_proj[depth_idx][:, second:second + block_width]], axis=1)
            result = jnp.dot(inputs, weights, preferred_element_type=jnp.float32)
            blocks_out[group_idx] = result[:, :block_width]
            blocks_out[group_idx + 4] = result[:, block_width:]
        grouped = jnp.concatenate(blocks_out, axis=1)
        current = (grouped * out_scale[depth_idx][None, :]).astype(jnp.bfloat16)
    return current
```

```python
import functools

import jax
import jax.numpy as jnp
from jax import lax
from jax.experimental import pallas as pl
from jax.experimental.pallas import tpu as pltpu
from jax.sharding import PartitionSpec as P

D = 4096
WIN = 16
LAYERS = 2
HALO = LAYERS * WIN


epsilon = 1e-06


def from_behind(block, axis, distance):
    devices = range(lax.axis_size(axis))
    route = [(i - distance, i) for i in devices if i - distance in devices]
    return lax.ppermute(block, axis, route)


def partner_2(value, axis, stride):
    mask = 2**stride
    pairs = [(source, source ^ mask) for source in range(lax.axis_size(axis))]
    return lax.ppermute(value, axis, pairs)


def normalize(current, gain_row):
    values = current.astype(jnp.float32)
    scaled = values * lax.rsqrt(jnp.mean(values * values, axis=-1, keepdims=True) + epsilon)
    return (scaled * gain_row[None, :]).astype(jnp.bfloat16)


def pool_block(extended, ext_flags, own_flags, proj_f32, windows, local_rows):
    window_sum = jnp.zeros_like(proj_f32)
    window_count = jnp.zeros_like(proj_f32)
    for offset in range(WIN):
        begin = WIN - 1 - offset
        shifted = extended[begin : begin + local_rows]
        same_doc = ext_flags[begin : begin + local_rows] == own_flags
        taken = same_doc[:, None] & (offset < windows)[None, :]
        window_sum = window_sum + jnp.where(taken, shifted, jnp.float32(0.0))
        window_count = window_count + taken.astype(jnp.float32)
    return (window_sum / window_count - proj_f32).astype(jnp.bfloat16)


def shards(tokens, doc_ids, norm_gain, in_proj, mix_proj, out_scale):
    local_rows = tokens.shape[0]
    local_width = tokens.shape[1]
    block_width = D // 8
    blocks_here = local_width // block_width
    tp_count = lax.axis_size("tp")
    half_bit = tp_count.bit_length() - 2
    tp_index = lax.axis_index("tp")
    chan_start = tp_index * local_width
    channels = chan_start + jnp.arange(local_width, dtype=jnp.int32)
    windows = jnp.left_shift(jnp.int32(2), channels // block_width % 4)
    low_side = tp_index < tp_count // 2
    doc_flags = (doc_ids + 1).astype(jnp.bfloat16)
    in_whole, mix_whole = (
        lax.all_gather(in_proj, "sp", axis=1, tiled=True),
        lax.all_gather(mix_proj, "sp", axis=1, tiled=True),
    )
    current = tokens
    for depth_idx in range(LAYERS):
        gathered = lax.all_gather(current, "tp", axis=1, tiled=True)
        normed = normalize(gathered, norm_gain[depth_idx])
        proj_sum = jnp.dot(normed, in_whole[depth_idx], preferred_element_type=jnp.float32)
        projected = proj_sum.astype(jnp.bfloat16)
        tail_rows, tail_flags = from_behind(
            (projected[local_rows - (WIN - 1) :], doc_flags[local_rows - (WIN - 1) :]), "sp", 1
        )
        extended = jnp.concatenate([tail_rows, projected], axis=0).astype(jnp.float32)
        ext_flags = jnp.concatenate([tail_flags, doc_flags], axis=0)
        pooled = pool_block(
            extended, ext_flags, doc_flags, projected.astype(jnp.float32), windows, local_rows
        )
        partner = partner_2(pooled, "tp", half_bit)
        low_part = jnp.where(low_side, pooled, partner)
        high_part = jnp.where(low_side, partner, pooled)
        group_inputs = [
            jnp.concatenate(
                [
                    low_part[:, block_idx * block_width : (block_idx + 1) * block_width],
                    high_part[:, block_idx * block_width : (block_idx + 1) * block_width],
                ],
                axis=1,
            )
            for block_idx in range(blocks_here)
        ]
        shard_rows = mix_whole[depth_idx]
        pieces_out = []
        for add_block_idx in range(blocks_here):
            add_inputs = group_inputs[add_block_idx]
            pieces_out.append(
                jnp.dot(
                    add_inputs,
                    shard_rows[:, add_block_idx * block_width : (add_block_idx + 1) * block_width],
                    preferred_element_type=jnp.float32,
                )
            )
        grouped = jnp.concatenate(pieces_out, axis=1)
        scale_row = lax.dynamic_slice_in_dim(out_scale[depth_idx], chan_start, local_width, 0)
        current = (grouped * scale_row[None, :]).astype(jnp.bfloat16)
    return current


SEG = 2


def peer_of(p, k):
    return (p // 2 + k // 2) % 2 * 2 + (p % 2 + k % 2) % 2


def place_of(sp):
    return sp % 2, sp // 2 % 2, sp // 4


def fused_kernel(
    own, tok, in_w, mix_w, gain, scale, out,
    xt, normed, acts, w_in, w_mix, acc, proj, docs, pooled, last,
    rx_in, rx_mix, y_in, y_mix, z_in, z_mix, tx_in, tx_mix,
    tok_rx, tok_prx, tok_tx, tok_ptx, halo, halo_tx, act_rx, act_prx, act_tx, act_ptx,
    pool_sem, out_rx, out_tx,
):
    sp = lax.axis_index("sp")
    c = lax.axis_index("tp")
    nsp = lax.axis_size("sp")
    x, y, z = place_of(sp)
    half_z, g = z // 2, x + 2 * (z % 2)
    seg = HALO + 2 * own
    total = SEG * seg
    width = w_in.shape[2]
    k_in, k_mix = in_w.shape[1], mix_w.shape[1]
    partner = (sp, 1 - c)

    def sp_at(p, row, upper):
        return 4 * (2 * upper + p // 2) + 2 * row + p % 2

    def peer(k):
        return (sp_at(peer_of(g, k), y, half_z), c)

    beside = (sp_at(g, 1 - y, half_z), c)
    across = (sp_at(g, y, 1 - half_z), c)
    behind = [4 * (2 * half_z + i) + 2 * y - 1 for i in range(SEG)]
    next_x, next_y, next_z = place_of(sp + 1)
    feeds = (x == 1) & (sp + 1 < nsp)

    def remote(src, dst, tx, rx, to):
        return pltpu.make_async_remote_copy(
            src_ref=src, dst_ref=dst, send_sem=tx, recv_sem=rx, device_id=to,
            device_id_type=pl.DeviceIdType.MESH,
        )

    barrier = pltpu.get_barrier_semaphore()

    def greet(to):
        pl.semaphore_signal(barrier, inc=1, device_id=to, device_id_type=pl.DeviceIdType.MESH)

    for k in (1, 2, 3):
        greet(peer(k))
    for to in (partner, beside, across):
        greet(to)
    for i in range(SEG):
        @pl.when(behind[i] >= 0)
        def _():
            greet((behind[i], c))

    @pl.when(feeds)
    def _():
        for p in range(4):
            greet((sp_at(p, next_y, next_z // 2), c))

    fed = [jnp.where(behind[i] >= 0, 1, 0) for i in range(SEG)]
    pl.semaphore_wait(barrier, 6 + fed[0] + fed[1] + jnp.where(feeds, 4, 0))

    def in_piece(l, s):
        return w_in.at[l, pl.ds(s * k_in, k_in), :]

    def mix_piece(l, s):
        return w_mix.at[l, pl.ds(s * k_mix, k_mix), :]

    kinds = {
        "in": (in_piece, in_w, rx_in, y_in, z_in, tx_in),
        "mix": (mix_piece, mix_w, rx_mix, y_mix, z_mix, tx_mix),
    }

    def own_weight(kind, l):
        piece, src, rx = kinds[kind][:3]
        return pltpu.make_async_copy(
            src.at[l, :, pl.ds(g * width, width)], piece(l, sp), rx.at[l, sp]
        )

    def give_weight(kind, l, k):
        piece, src, rx, _, _, tx = kinds[kind]
        return remote(
            src.at[l, :, pl.ds(peer_of(g, k) * width, width)], piece(l, sp),
            tx.at[l, k], rx.at[l, sp], peer(k),
        )

    def to_beside(kind, l, s):
        piece, _, rx, tx = kinds[kind][:4]
        return remote(piece(l, s), piece(l, s), tx.at[l, s], rx.at[l, s], beside)

    def to_across(kind, l, s):
        piece, _, rx, _, tx = kinds[kind][:5]
        return remote(piece(l, s), piece(l, s), tx.at[l, s], rx.at[l, s], across)

    def arrived(kind, l, s):
        piece, _, rx = kinds[kind][:3]
        remote(piece(l, s), piece(l, s), rx.at[l, s], rx.at[l, s], partner).wait_recv()

    def home(k):
        return sp_at(peer_of(g, k), y, half_z)

    def away(k):
        return sp_at(peer_of(g, k), y, 1 - half_z)

    def pump_home(kind, l, ks=range(4)):
        for k in ks:
            if k == 0:
                own_weight(kind, l).wait()
            else:
                arrived(kind, l, home(k))
            to_across(kind, l, home(k)).start()
            to_beside(kind, l, home(k)).start()

    def pump_away(kind, l, ks=range(4)):
        for k in ks:
            arrived(kind, l, away(k))
            to_beside(kind, l, away(k)).start()

    def from_beside(kind, l):
        for k in range(4):
            arrived(kind, l, sp_at(peer_of(g, k), 1 - y, half_z))
            arrived(kind, l, sp_at(peer_of(g, k), 1 - y, 1 - half_z))

    def start_weights(kind, l):
        own_weight(kind, l).start()
        for k in (1, 2, 3):
            give_weight(kind, l, k).start()

    def row_of(q):
        return q // 2 * seg + HALO + q % 2 * own

    def rows_of(q):
        return pl.ds(pl.multiple_of(row_of(q), 16), own)

    def halo_at(side, i):
        return xt.at[side, pl.ds(pl.multiple_of(i * seg, 16), HALO), :]

    def halo_send(p):
        to = (sp_at(p, next_y, next_z // 2), c)
        tail = tok.at[pl.ds(own - HALO, HALO), :]
        return remote(tail, halo_at(c, next_z % 2), halo_tx.at[p], halo.at[next_z % 2], to)

    def halo_part(i):
        return remote(halo_at(c, i), halo_at(c, i), halo_tx.at[4 + i], halo.at[2 + i], partner)

    start_weights("in", 0)
    tok_here = pltpu.make_async_copy(tok, xt.at[c, rows_of(g), :], tok_rx.at[0])
    tok_here.start()
    tok_sent = [remote(tok, xt.at[c, rows_of(g), :], tok_ptx.at[0], tok_prx.at[0], partner)]
    for k in (1, 2):
        tok_sent.append(
            remote(tok, xt.at[c, rows_of(g), :], tok_tx.at[k], tok_rx.at[k], peer(k))
        )
    for copy in tok_sent:
        copy.start()

    @pl.when(feeds)
    def _():
        for p in range(4):
            halo_send(p).start()

    @pl.when(behind[0] < 0)
    def _():
        xt[:, 0:HALO, :] = jnp.zeros((2, HALO, xt.shape[2]), xt.dtype)

    docs[0:16, :] = jnp.zeros((16, 128), jnp.float32)
    proj[0:16, :] = jnp.zeros((16, width), proj.dtype)

    def spread(block, rx, tx, prx, ptx, sent):
        for k in (2, 1):
            spot = block(c, peer_of(g, k))
            remote(spot, spot, rx.at[k], rx.at[k], partner).wait_recv()
            if k == 2:
                copy = remote(spot, spot, tx.at[3], rx.at[3], peer(1))
                copy.start()
                sent.append(copy)
            copy = remote(spot, spot, ptx.at[k], prx.at[k], partner)
            copy.start()
            sent.append(copy)

    def spread_end(block, rx, prx, ptx, sent):
        spot = block(c, peer_of(g, 3))
        remote(spot, spot, rx.at[3], rx.at[3], partner).wait_recv()
        copy = remote(spot, spot, ptx.at[3], prx.at[3], partner)
        copy.start()
        sent.append(copy)

    def from_partner(block, prx, k):
        spot = block(1 - c, peer_of(g, k))
        remote(spot, spot, prx.at[k], prx.at[k], partner).wait_recv()

    def tok_block(side, q):
        return xt.at[side, rows_of(q), :]

    half = 4 * width
    step = 16
    tile = total // 2
    chunk = 32

    def normalize_rows(l, load, start, count):
        def body(i, carry):
            r = pl.ds(pl.multiple_of(start + i * step, step), step)
            squares = jnp.zeros((step, 128), jnp.float32)
            for j in range(8):
                v = load(j, r).astype(jnp.float32)
                v = v * v
                for q in range(width // 128):
                    squares = squares + v[:, q * 128 : (q + 1) * 128]
            mean = jnp.sum(squares, axis=-1, keepdims=True) * (1.0 / (8 * width))
            factor = lax.rsqrt(mean + epsilon)
            for j in range(8):
                v = load(j, r).astype(jnp.float32) * factor
                normed[r, j * width : (j + 1) * width] = (
                    v * gain[l : l + 1, j * width : (j + 1) * width]
                ).astype(jnp.bfloat16)
            return carry

        lax.fori_loop(0, count // step, body, 0)

    def load_tokens(j, r):
        h = j // 4
        return xt[h, r, (j % 4) * width : (j % 4 + 1) * width]

    def load_acts(j, r):
        return acts[j, r, :]

    def project(l):
        for m in range(2):
            r = slice(m * tile, (m + 1) * tile)

            def body(i, carry):
                ks = pl.ds(pl.multiple_of(i * width, width), width)
                acc[r, :] += jnp.dot(
                    normed[r, ks], w_in[l, ks, :], preferred_element_type=jnp.float32
                )
                return carry

            acc[r, :] = jnp.dot(
                normed[r, 0:width], w_in[l, 0:width, :], preferred_element_type=jnp.float32
            )
            lax.fori_loop(1, 8, body, 0)
            proj[16 + m * tile : 16 + (m + 1) * tile, :] = acc[r, :].astype(jnp.bfloat16)

    def add_piece(s):
        s = jnp.int32(s)
        ks = pl.ds(pl.multiple_of(s * k_in, k_in), k_in)
        for m in range(2):
            r = slice(m * tile, (m + 1) * tile)
            acc[r, :] += jnp.dot(
                normed[r, ks], w_in[1, ks, :], preferred_element_type=jnp.float32
            )

    def add_group(row, upper):
        def body(k, carry):
            add_piece(sp_at(k, row, upper))
            return carry

        lax.fori_loop(0, 4, body, 0)

    def pool(flags):
        def body(i, carry):
            base = pl.multiple_of(i * chunk, chunk)
            ext = pl.ds(base, chunk + 16)
            d = docs[ext, :]
            same = []
            count = jnp.ones_like(d)
            for j in range(4):
                ok = jnp.where(pltpu.roll(d, 2**j, 0) == d, flags[j], 0.0)
                same.append(ok)
                count = count + ok * pltpu.roll(count, 2**j, 0)
            for q in range(width // 128):
                cols = slice(q * 128, (q + 1) * 128)
                p = proj[ext, cols].astype(jnp.float32)
                total_sum = p
                for j in range(4):
                    total_sum = total_sum + same[j] * pltpu.roll(total_sum, 2**j, 0)
                v = total_sum / count - p
                pooled[c, pl.ds(base, chunk), cols] = v[16:, :].astype(jnp.bfloat16)
            return carry

        lax.fori_loop(0, total // chunk, body, 0)

    flags = [jnp.where(g >= j, jnp.float32(1.0), jnp.float32(0.0)) for j in range(4)]

    def swap_pooled(l):
        here = pooled.at[c]
        return remote(here, here, pool_sem.at[l, 0], pool_sem.at[l, 1], partner)

    def pooled_arrived(l):
        there = pooled.at[1 - c]
        remote(there, there, pool_sem.at[l, 1], pool_sem.at[l, 1], partner).wait_recv()

    def mix(l, store):
        for m in range(2):
            r = slice(m * tile, (m + 1) * tile)
            y = jnp.dot(pooled[0, r, :], w_mix[l, 0:width, :], preferred_element_type=jnp.float32)
            y = y + jnp.dot(
                pooled[1, r, :], w_mix[l, width : 2 * width, :], preferred_element_type=jnp.float32
            )
            store(r, (y * scale[l : l + 1, :]).astype(jnp.bfloat16))

    def normalize_block(k):
        start = pl.multiple_of(row_of(peer_of(g, k)), 16)
        normalize_rows(0, load_tokens, start, own)

    pump_home("in", 0)
    tok_here.wait()
    spread(tok_block, tok_rx, tok_tx, tok_prx, tok_ptx, tok_sent)
    start_weights("mix", 0)
    start_weights("in", 1)
    start_weights("mix", 1)
    pump_away("in", 0)

    for i in range(SEG):
        @pl.when(behind[i] >= 0)
        def _():
            spot = halo_at(c, i)
            remote(spot, spot, halo.at[i], halo.at[i], partner).wait_recv()
            halo_part(i).start()

    from_partner(tok_block, tok_prx, 0)
    normalize_block(0)
    pump_home("mix", 0)
    for k in (2, 1):
        from_partner(tok_block, tok_prx, k)
        normalize_block(k)
    pump_away("mix", 0)
    spread_end(tok_block, tok_rx, tok_prx, tok_ptx, tok_sent)
    pump_home("in", 1)
    for i in range(SEG):
        @pl.when(behind[i] >= 0)
        def _():
            spot = halo_at(1 - c, i)
            remote(spot, spot, halo.at[2 + i], halo.at[2 + i], partner).wait_recv()

        normalize_rows(0, load_tokens, i * seg, HALO)
    pump_home("mix", 1)
    from_partner(tok_block, tok_prx, 3)
    normalize_block(3)
    docs[16 : 16 + total, :] = xt[0, :, half : half + 128].astype(jnp.float32)
    from_beside("in", 0)
    project(0)
    pool(flags)
    swap_pooled(0).start()
    from_beside("mix", 0)
    pump_away("in", 1)
    pooled_arrived(0)
    mine = g + 4 * c

    def store_acts(r, v):
        acts[mine, r, :] = v

    mix(0, store_acts)
    here = acts.at[mine]
    act_sent = [remote(here, here, act_ptx.at[0], act_prx.at[0], partner)]
    for k in (1, 2):
        act_sent.append(remote(here, here, act_tx.at[k], act_rx.at[k], peer(k)))
    for copy in act_sent[1:] + act_sent[:1]:
        copy.start()

    def act_block(side, q):
        return acts.at[q + 4 * side]

    pump_away("mix", 1)
    spread(act_block, act_rx, act_tx, act_prx, act_ptx, act_sent)
    spread_end(act_block, act_rx, act_prx, act_ptx, act_sent)
    for k in range(4):
        from_partner(act_block, act_prx, k)
    normalize_rows(1, load_acts, 0, total)
    acc[...] = jnp.zeros_like(acc)
    add_group(y, half_z)
    add_group(y, 1 - half_z)
    from_beside("in", 1)
    add_group(1 - y, half_z)
    add_group(1 - y, 1 - half_z)
    proj[16 : 16 + total, :] = acc[...].astype(jnp.bfloat16)
    swap_pooled(0).wait_send()
    pool(flags)
    swap_pooled(1).start()
    from_beside("mix", 1)
    pooled_arrived(1)

    def store_last(r, v):
        last[r, :] = v

    mix(1, store_last)
    place = out.at[:, pl.ds(g * width, width)]
    for k in (1, 2, 3):
        remote(
            last.at[rows_of(peer_of(g, k)), :], place, out_tx.at[k], out_rx.at[k], peer(k)
        ).start()
    keep = pltpu.make_async_copy(last.at[rows_of(g), :], place, out_rx.at[0])
    keep.start()

    swap_pooled(1).wait_send()
    for kind in ("in", "mix"):
        for l in range(2):
            for k in (1, 2, 3):
                give_weight(kind, l, k).wait_send()
            for k in range(4):
                to_across(kind, l, home(k)).wait_send()
                to_beside(kind, l, home(k)).wait_send()
                to_beside(kind, l, away(k)).wait_send()

    @pl.when(feeds)
    def _():
        for p in range(4):
            halo_send(p).wait_send()

    for i in range(SEG):
        @pl.when(behind[i] >= 0)
        def _():
            halo_part(i).wait_send()

    for copy in tok_sent + act_sent:
        copy.wait_send()
    for k in (1, 2, 3):
        spot = out.at[:, pl.ds(peer_of(g, k) * width, width)]
        remote(
            last.at[rows_of(peer_of(g, k)), :], spot, out_tx.at[k], out_rx.at[k], peer(k)
        ).wait()
    keep.wait()


def fused_shards(tokens, doc_ids, norm_gain, in_proj, mix_proj, out_scale):
    own, local_width = tokens.shape
    width = local_width // 4
    nsp = lax.axis_size("sp")
    total = SEG * (HALO + 2 * own)
    tile_docs = jnp.broadcast_to((doc_ids + 1).astype(jnp.bfloat16)[:, None], (own, 128))
    tok = jnp.concatenate([tokens, tile_docs], axis=1)
    x, _, z = place_of(lax.axis_index("sp"))
    block = x + 2 * (z % 2) + 4 * lax.axis_index("tp")
    scale = lax.dynamic_slice_in_dim(out_scale, block * width, width, 1)
    any_spec = pl.BlockSpec(memory_space=pl.ANY)
    vmem_spec = pl.BlockSpec(memory_space=pltpu.VMEM)
    bf16, f32 = jnp.bfloat16, jnp.float32
    dma = pltpu.SemaphoreType.DMA
    scratch = [
        pltpu.VMEM((2, total, local_width + 128), bf16),
        pltpu.VMEM((total, 8 * width), bf16),
        pltpu.VMEM((8, total, width), bf16),
        pltpu.VMEM((2, 8 * width, width), bf16),
        pltpu.VMEM((2, 2 * width, width), bf16),
        pltpu.VMEM((total, width), f32),
        pltpu.VMEM((16 + total, width), bf16),
        pltpu.VMEM((16 + total, 128), f32),
        pltpu.VMEM((2, total, width), bf16),
        pltpu.VMEM((total, width), bf16),
    ]
    scratch += [dma((2, nsp)) for _ in range(6)] + [dma((2, 4)) for _ in range(2)]
    scratch += [dma((5,)) for _ in range(4)] + [dma((4,)), dma((6,))]
    scratch += [dma((5,)) for _ in range(4)] + [dma((2, 2)), dma((4,)), dma((4,))]
    return pl.pallas_call(
        functools.partial(fused_kernel, own),
        out_shape=jax.ShapeDtypeStruct((own, local_width), bf16),
        in_specs=[any_spec, any_spec, any_spec, vmem_spec, vmem_spec],
        out_specs=any_spec,
        scratch_shapes=scratch,
        compiler_params=pltpu.CompilerParams(
            collective_id=0, has_side_effects=True, vmem_limit_bytes=60 * 1024 * 1024
        ),
    )(tok, in_proj, mix_proj, norm_gain, scale)


def solution(mesh):
    placed = (P("sp", "tp"), P("sp"), P(), P(None, "sp", "tp"), P(None, "sp", "tp"), P())
    body = fused_shards if mesh.shape["tp"] == 2 and mesh.shape["sp"] == 16 else shards
    return jax.shard_map(
        body, mesh=mesh, in_specs=placed, out_specs=P("sp", "tp"), check_vma=False
    )
```

```python
import functools

import jax
import jax.numpy as jnp
from jax import lax
from jax.experimental import pallas as pl
from jax.experimental.pallas import tpu as pltpu
from jax.sharding import PartitionSpec as P

D = 4096
WIN = 16
LAYERS = 2
HALO = LAYERS * WIN


epsilon = 1e-06


def from_behind(block, axis, distance):
    devices = range(lax.axis_size(axis))
    route = [(i - distance, i) for i in devices if i - distance in devices]
    return lax.ppermute(block, axis, route)


def partner_2(value, axis, stride):
    mask = 2**stride
    pairs = [(source, source ^ mask) for source in range(lax.axis_size(axis))]
    return lax.ppermute(value, axis, pairs)


def normalize(current, gain_row):
    values = current.astype(jnp.float32)
    scaled = values * lax.rsqrt(jnp.mean(values * values, axis=-1, keepdims=True) + epsilon)
    return (scaled * gain_row[None, :]).astype(jnp.bfloat16)


def pool_block(extended, ext_flags, own_flags, proj_f32, windows, local_rows):
    window_sum = jnp.zeros_like(proj_f32)
    window_count = jnp.zeros_like(proj_f32)
    for offset in range(WIN):
        begin = WIN - 1 - offset
        shifted = extended[begin : begin + local_rows]
        same_doc = ext_flags[begin : begin + local_rows] == own_flags
        taken = same_doc[:, None] & (offset < windows)[None, :]
        window_sum = window_sum + jnp.where(taken, shifted, jnp.float32(0.0))
        window_count = window_count + taken.astype(jnp.float32)
    return (window_sum / window_count - proj_f32).astype(jnp.bfloat16)


def shards(tokens, doc_ids, norm_gain, in_proj, mix_proj, out_scale):
    local_rows = tokens.shape[0]
    local_width = tokens.shape[1]
    block_width = D // 8
    blocks_here = local_width // block_width
    tp_count = lax.axis_size("tp")
    half_bit = tp_count.bit_length() - 2
    tp_index = lax.axis_index("tp")
    chan_start = tp_index * local_width
    channels = chan_start + jnp.arange(local_width, dtype=jnp.int32)
    windows = jnp.left_shift(jnp.int32(2), channels // block_width % 4)
    low_side = tp_index < tp_count // 2
    doc_flags = (doc_ids + 1).astype(jnp.bfloat16)
    in_whole, mix_whole = (
        lax.all_gather(in_proj, "sp", axis=1, tiled=True),
        lax.all_gather(mix_proj, "sp", axis=1, tiled=True),
    )
    current = tokens
    for depth_idx in range(LAYERS):
        gathered = lax.all_gather(current, "tp", axis=1, tiled=True)
        normed = normalize(gathered, norm_gain[depth_idx])
        proj_sum = jnp.dot(normed, in_whole[depth_idx], preferred_element_type=jnp.float32)
        projected = proj_sum.astype(jnp.bfloat16)
        tail_rows, tail_flags = from_behind(
            (projected[local_rows - (WIN - 1) :], doc_flags[local_rows - (WIN - 1) :]), "sp", 1
        )
        extended = jnp.concatenate([tail_rows, projected], axis=0).astype(jnp.float32)
        ext_flags = jnp.concatenate([tail_flags, doc_flags], axis=0)
        pooled = pool_block(
            extended, ext_flags, doc_flags, projected.astype(jnp.float32), windows, local_rows
        )
        partner = partner_2(pooled, "tp", half_bit)
        low_part = jnp.where(low_side, pooled, partner)
        high_part = jnp.where(low_side, partner, pooled)
        group_inputs = [
            jnp.concatenate(
                [
                    low_part[:, block_idx * block_width : (block_idx + 1) * block_width],
                    high_part[:, block_idx * block_width : (block_idx + 1) * block_width],
                ],
                axis=1,
            )
            for block_idx in range(blocks_here)
        ]
        shard_rows = mix_whole[depth_idx]
        pieces_out = []
        for add_block_idx in range(blocks_here):
            add_inputs = group_inputs[add_block_idx]
            pieces_out.append(
                jnp.dot(
                    add_inputs,
                    shard_rows[:, add_block_idx * block_width : (add_block_idx + 1) * block_width],
                    preferred_element_type=jnp.float32,
                )
            )
        grouped = jnp.concatenate(pieces_out, axis=1)
        scale_row = lax.dynamic_slice_in_dim(out_scale[depth_idx], chan_start, local_width, 0)
        current = (grouped * scale_row[None, :]).astype(jnp.bfloat16)
    return current


PARTS = ((0, 0, 4), (1, 0, 2), (1, 2, 1), (1, 3, 1))


def peer_of(g, k):
    return (g // 2 + k // 2) % 2 * 2 + (g % 2 + k % 2) % 2


def fused_kernel(
    nz, own, tok, in_w, mix_w, gain, scale, out,
    xt, normed, acts, w_in, w_mix, acc, proj, docs, pooled, last,
    rx_in, rx_mix, up_in, up_mix, dn_in, dn_mix, tx_in, tx_mix,
    tok_rx, tok_prx, tok_tx, tok_ptx, halo, halo_tx, act_rx, act_prx, act_tx, act_ptx,
    pool_sem, out_rx, out_tx,
):
    sp = lax.axis_index("sp")
    c = lax.axis_index("tp")
    z, g = sp // 4, sp % 4
    total = HALO + 4 * own
    width = w_in.shape[2]
    k_in, k_mix = in_w.shape[1], mix_w.shape[1]
    partner = (sp, 1 - c)

    def peer(k):
        return (z * 4 + peer_of(g, k), c)

    def remote(src, dst, tx, rx, to):
        return pltpu.make_async_remote_copy(
            src_ref=src, dst_ref=dst, send_sem=tx, recv_sem=rx, device_id=to,
            device_id_type=pl.DeviceIdType.MESH,
        )

    barrier = pltpu.get_barrier_semaphore()

    def greet(to):
        pl.semaphore_signal(barrier, inc=1, device_id=to, device_id_type=pl.DeviceIdType.MESH)

    for k in (1, 2, 3):
        greet(peer(k))
    greet(partner)

    @pl.when(z > 0)
    def _():
        greet((sp - 4, c))

    @pl.when(z < nz - 1)
    def _():
        greet((sp + 4, c))

    ends = jnp.where(z > 0, 1, 0) + jnp.where(z < nz - 1, 1, 0)
    pl.semaphore_wait(barrier, 4 + ends)

    def in_piece(l, s):
        return w_in.at[l, pl.ds(s * k_in, k_in), :]

    def columns(kind, l, block):
        if kind == "in":
            return l, pl.ds(block * width, width)
        layer, first, count = PARTS[l]
        unit = width // 4
        return layer, pl.ds(block * width + first * unit, count * unit)

    def mix_piece(l, s):
        layer, cols = columns("mix", l, 0)
        return w_mix.at[layer, pl.ds(s * k_mix, k_mix), cols]

    kinds = {
        "in": (in_piece, in_w, rx_in, up_in, dn_in, tx_in),
        "mix": (mix_piece, mix_w, rx_mix, up_mix, dn_mix, tx_mix),
    }

    def given(kind, l, block):
        layer, cols = columns(kind, l, block)
        return kinds[kind][1].at[layer, :, cols]

    def own_weight(kind, l):
        piece, _, rx = kinds[kind][:3]
        return pltpu.make_async_copy(given(kind, l, g), piece(l, sp), rx.at[l, sp])

    def give_weight(kind, l, k):
        piece, _, rx, _, _, tx = kinds[kind]
        return remote(
            given(kind, l, peer_of(g, k)), piece(l, sp), tx.at[l, k], rx.at[l, sp], peer(k),
        )

    def relay(kind, l, s, up, src=None):
        piece, _, rx, up_tx, dn_tx, _ = kinds[kind]
        tx = up_tx if up else dn_tx
        to = sp + 4 if up else sp - 4
        src = piece(l, s) if src is None else src
        return remote(src, piece(l, s), tx.at[l, s], rx.at[l, s], (to, c))

    def arrived(kind, l, s):
        piece, _, rx = kinds[kind][:3]
        remote(piece(l, s), piece(l, s), rx.at[l, s], rx.at[l, s], partner).wait_recv()

    def send_relay(kind, l, s, up, src=None):
        @pl.when((z < nz - 1) if up else (z > 0))
        def _():
            relay(kind, l, s, up, src).start()

    def pump_plane(kind, l):
        if kind == "mix" or l:
            own_weight(kind, l).wait()
            send_relay(kind, l, sp, True)
            send_relay(kind, l, sp, False)
        for k in (1, 2, 3):
            s = z * 4 + peer_of(g, k)
            arrived(kind, l, s)
            send_relay(kind, l, s, True)
            send_relay(kind, l, s, False)

    def pump_far(kind, l, far, ks=range(4)):
        for k in ks:
            @pl.when(z >= far)
            def _():
                s = (z - far) * 4 + peer_of(g, k)
                arrived(kind, l, s)
                send_relay(kind, l, s, True)

            @pl.when(z + far < nz)
            def _():
                s = (z + far) * 4 + peer_of(g, k)
                arrived(kind, l, s)
                send_relay(kind, l, s, False)

    def pump_line(kind, l):
        for far in range(1, nz):
            pump_far(kind, l, far)

    def start_weights(kind, l):
        own_weight(kind, l).start()
        for k in (1, 2, 3):
            give_weight(kind, l, k).start()

    def rows_of(q):
        return pl.ds(HALO + q * own, own)

    halo_here = xt.at[c, pl.ds(0, HALO), :]
    tail = tok.at[pl.ds(own - HALO, HALO), :]
    halo_up = remote(tail, halo_here, halo_tx.at[0], halo.at[0], (sp + 4, c))
    halo_peer = {k: remote(halo_here, halo_here, halo_tx.at[k], halo.at[0], peer(k)) for k in (1, 2, 3)}
    halo_part = remote(halo_here, halo_here, halo_tx.at[4], halo.at[1], partner)

    @pl.when((z < nz - 1) & (g == 3))
    def _():
        halo_up.start()

    for up in (True, False):
        send_relay("in", 0, sp, up, given("in", 0, g))
    start_weights("in", 0)
    tok_here = pltpu.make_async_copy(tok, xt.at[c, rows_of(g), :], tok_rx.at[0])
    tok_here.start()
    tok_sent = [remote(tok, xt.at[c, rows_of(g), :], tok_ptx.at[0], tok_prx.at[0], partner)]
    for k in (1, 2):
        tok_sent.append(
            remote(tok, xt.at[c, rows_of(g), :], tok_tx.at[k], tok_rx.at[k], peer(k))
        )
    for copy in tok_sent:
        copy.start()

    @pl.when(z == 0)
    def _():
        xt[:, 0:HALO, :] = jnp.zeros((2, HALO, xt.shape[2]), xt.dtype)

    docs[0:16, :] = jnp.zeros((16, 128), jnp.float32)
    proj[0:16, :] = jnp.zeros((16, width), proj.dtype)

    def spread(block, rx, tx, prx, ptx, sent):
        for k in (1, 2):
            spot = block(c, peer_of(g, k))
            remote(spot, spot, rx.at[k], rx.at[k], partner).wait_recv()
        for k in (1, 2):
            part = half_of(block(c, peer_of(g, k)), k)
            copy = remote(part, part, tx.at[2 + k], rx.at[2 + k], peer(3 - k))
            copy.start()
            sent.append(copy)
        for k in (1, 2):
            spot = block(c, peer_of(g, k))
            copy = remote(spot, spot, ptx.at[k], prx.at[k], partner)
            copy.start()
            sent.append(copy)

    def spread_end(block, rx, prx, ptx, sent):
        spot = block(c, peer_of(g, 3))
        for k in (1, 2):
            part = half_of(spot, k)
            remote(part, part, rx.at[2 + k], rx.at[2 + k], partner).wait_recv()
        copy = remote(spot, spot, ptx.at[3], prx.at[3], partner)
        copy.start()
        sent.append(copy)

    def from_partner(block, prx, k):
        spot = block(1 - c, peer_of(g, k))
        remote(spot, spot, prx.at[k], prx.at[k], partner).wait_recv()

    def half_of(spot, k):
        n = spot.shape[0] // 2
        return spot.at[pl.ds((k - 1) * n, n), :]

    def tok_block(side, q):
        return xt.at[side, rows_of(q), :]

    half = 4 * width
    step = 16
    tile = total // 2
    chunk = 32

    def normalize_rows(l, load, start, count):
        def body(i, carry):
            r = pl.ds(pl.multiple_of(start + i * step, step), step)
            squares = jnp.zeros((step, 128), jnp.float32)
            for j in range(8):
                v = load(j, r).astype(jnp.float32)
                v = v * v
                for q in range(width // 128):
                    squares = squares + v[:, q * 128 : (q + 1) * 128]
            mean = jnp.sum(squares, axis=-1, keepdims=True) * (1.0 / (8 * width))
            factor = lax.rsqrt(mean + epsilon)
            for j in range(8):
                v = load(j, r).astype(jnp.float32) * factor
                normed[r, j * width : (j + 1) * width] = (
                    v * gain[l : l + 1, j * width : (j + 1) * width]
                ).astype(jnp.bfloat16)
            return carry

        lax.fori_loop(0, count // step, body, 0)

    def load_tokens(j, r):
        h = j // 4
        return xt[h, r, (j % 4) * width : (j % 4 + 1) * width]

    def load_acts(j, r):
        return acts[j, r, :]

    def project(l):
        for m in range(2):
            r = slice(m * tile, (m + 1) * tile)

            def body(i, carry):
                ks = pl.ds(pl.multiple_of(i * width, width), width)
                acc[r, :] += jnp.dot(
                    normed[r, ks], w_in[l, ks, :], preferred_element_type=jnp.float32
                )
                return carry

            acc[r, :] = jnp.dot(
                normed[r, 0:width], w_in[l, 0:width, :], preferred_element_type=jnp.float32
            )
            lax.fori_loop(1, 8, body, 0)
            proj[16 + m * tile : 16 + (m + 1) * tile, :] = acc[r, :].astype(jnp.bfloat16)

    def add_piece(s):
        ks = pl.ds(pl.multiple_of(s * k_in, k_in), k_in)
        for m in range(2):
            r = slice(m * tile, (m + 1) * tile)
            acc[r, :] += jnp.dot(
                normed[r, ks], w_in[1, ks, :], preferred_element_type=jnp.float32
            )

    def add_plane(src):
        def body(k, carry):
            add_piece(src * 4 + k)
            return carry

        lax.fori_loop(0, 4, body, 0)

    def pool(flags):
        def body(i, carry):
            base = pl.multiple_of(i * chunk, chunk)
            ext = pl.ds(base, chunk + 16)
            d = docs[ext, :]
            same = []
            count = jnp.ones_like(d)
            for j in range(4):
                ok = jnp.where(pltpu.roll(d, 2**j, 0) == d, flags[j], 0.0)
                same.append(ok)
                count = count + ok * pltpu.roll(count, 2**j, 0)
            for q in range(width // 128):
                cols = slice(q * 128, (q + 1) * 128)
                p = proj[ext, cols].astype(jnp.float32)
                total_sum = p
                for j in range(4):
                    total_sum = total_sum + same[j] * pltpu.roll(total_sum, 2**j, 0)
                v = total_sum / count - p
                pooled[c, pl.ds(base, chunk), cols] = v[16:, :].astype(jnp.bfloat16)
            return carry

        lax.fori_loop(0, total // chunk, body, 0)

    flags = [jnp.where(g >= j, jnp.float32(1.0), jnp.float32(0.0)) for j in range(4)]

    def swap_pooled(l):
        here = pooled.at[c]
        return remote(here, here, pool_sem.at[l, 0], pool_sem.at[l, 1], partner)

    def pooled_arrived(l):
        there = pooled.at[1 - c]
        remote(there, there, pool_sem.at[l, 1], pool_sem.at[l, 1], partner).wait_recv()

    def mix(part, store):
        l, cols = columns("mix", part, 0)
        for m in range(2):
            r = slice(m * tile, (m + 1) * tile)
            y = jnp.dot(
                pooled[0, r, :], w_mix[l, 0:width, cols], preferred_element_type=jnp.float32
            )
            y = y + jnp.dot(
                pooled[1, r, :], w_mix[l, width : 2 * width, cols],
                preferred_element_type=jnp.float32,
            )
            store(r, cols, (y * scale[l : l + 1, cols]).astype(jnp.bfloat16))

    def normalize_block(k):
        start = pl.multiple_of(HALO + peer_of(g, k) * own, 16)
        normalize_rows(0, load_tokens, start, own)

    pump_plane("in", 0)

    @pl.when((z > 0) & (g == 3))
    def _():
        remote(halo_here, halo_here, halo.at[0], halo.at[0], partner).wait_recv()
        halo_part.start()
        for k in (1, 2, 3):
            halo_peer[k].start()

    pump_far("in", 0, 1)
    tok_here.wait()
    from_partner(tok_block, tok_prx, 0)
    normalize_block(0)
    for far in range(2, nz - 1):
        pump_far("in", 0, far)
    spread(tok_block, tok_rx, tok_tx, tok_prx, tok_ptx, tok_sent)
    start_weights("mix", 0)
    start_weights("in", 1)
    for part in (1, 2, 3):
        start_weights("mix", part)

    @pl.when((z > 0) & (g != 3))
    def _():
        remote(halo_here, halo_here, halo.at[0], halo.at[0], partner).wait_recv()
        halo_part.start()

    for k in (1, 2):
        from_partner(tok_block, tok_prx, k)
        normalize_block(k)

    @pl.when(z > 0)
    def _():
        spot = xt.at[1 - c, pl.ds(0, HALO), :]
        remote(spot, spot, halo.at[1], halo.at[1], partner).wait_recv()

    normalize_rows(0, load_tokens, 0, HALO)
    spread_end(tok_block, tok_rx, tok_prx, tok_ptx, tok_sent)
    pump_plane("mix", 0)
    from_partner(tok_block, tok_prx, 3)
    normalize_block(3)
    docs[16 : 16 + total, :] = xt[0, :, half : half + 128].astype(jnp.float32)
    pump_far("in", 0, nz - 1)
    for far in range(1, nz - 1):
        pump_far("mix", 0, far)
    own_weight("in", 0).wait()
    project(0)
    pump_plane("in", 1)
    pool(flags)
    swap_pooled(0).start()
    pump_far("mix", 0, nz - 1)
    for part in (1, 2, 3):
        pump_plane("mix", part)
    pooled_arrived(0)
    mine = g + 4 * c

    def store_acts(r, cols, v):
        acts[mine, r, cols] = v

    mix(0, store_acts)
    here = acts.at[mine]
    act_sent = [remote(here, here, act_ptx.at[0], act_prx.at[0], partner)]
    for k in (1, 2):
        act_sent.append(remote(here, here, act_tx.at[k], act_rx.at[k], peer(k)))
    for copy in act_sent[1:] + act_sent[:1]:
        copy.start()

    def act_block(side, q):
        return acts.at[q + 4 * side]

    pump_far("in", 1, 1)
    for far in range(2, nz - 1):
        pump_far("in", 1, far, range(2))
    spread(act_block, act_rx, act_tx, act_prx, act_ptx, act_sent)
    for far in range(2, nz - 1):
        pump_far("in", 1, far, range(2, 4))
    spread_end(act_block, act_rx, act_prx, act_ptx, act_sent)
    for k in range(4):
        from_partner(act_block, act_prx, k)
    normalize_rows(1, load_acts, 0, total)
    acc[...] = jnp.zeros_like(acc)
    add_plane(z)
    for far in range(1, nz - 1):
        @pl.when(z >= far)
        def _():
            add_plane(z - far)

        @pl.when(z + far < nz)
        def _():
            add_plane(z + far)

    @pl.when((z == 0) | (z == nz - 1))
    def _():
        def body(k, carry):
            s = (nz - 1 - z) * 4 + peer_of(g, k)
            arrived("in", 1, s)
            add_piece(s)
            return carry

        lax.fori_loop(0, 4, body, 0)

    proj[16 : 16 + total, :] = acc[...].astype(jnp.bfloat16)
    swap_pooled(0).wait_send()
    pool(flags)
    swap_pooled(1).start()
    def store_last(r, cols, v):
        last[r, cols] = v

    def out_copy(part, k):
        _, place = columns("mix", part, g)
        _, cols = columns("mix", part, 0)
        src = last.at[rows_of(peer_of(g, k)), cols]
        dst = out.at[:, place]
        if k == 0:
            return pltpu.make_async_copy(src, dst, out_rx.at[part, 0])
        return remote(src, dst, out_tx.at[part, k], out_rx.at[part, k], peer(k))

    for part in (1, 2, 3):
        pump_line("mix", part)
        if part == 1:
            pooled_arrived(1)
        mix(part, store_last)
        for k in (1, 2, 3, 0):
            out_copy(part, k).start()

    swap_pooled(1).wait_send()
    for kind in ("in", "mix"):
        for l in range(2 if kind == "in" else len(PARTS)):
            for k in (1, 2, 3):
                give_weight(kind, l, k).wait_send()
            for src in range(nz):
                for k in range(4):
                    s = src * 4 + k

                    @pl.when((z >= src) & (z < nz - 1))
                    def _():
                        relay(kind, l, s, True).wait_send()

                    @pl.when((z <= src) & (z > 0))
                    def _():
                        relay(kind, l, s, False).wait_send()

    @pl.when((z < nz - 1) & (g == 3))
    def _():
        halo_up.wait_send()

    @pl.when(z > 0)
    def _():
        halo_part.wait_send()

        @pl.when(g == 3)
        def _():
            for k in (1, 2, 3):
                halo_peer[k].wait_send()

    for copy in tok_sent + act_sent:
        copy.wait_send()
    for part in (1, 2, 3):
        for k in (1, 2, 3):
            _, place = columns("mix", part, peer_of(g, k))
            _, cols = columns("mix", part, 0)
            remote(
                last.at[rows_of(peer_of(g, k)), cols], out.at[:, place],
                out_tx.at[part, k], out_rx.at[part, k], peer(k),
            ).wait()
        out_copy(part, 0).wait()


def fused_shards(tokens, doc_ids, norm_gain, in_proj, mix_proj, out_scale):
    own, local_width = tokens.shape
    width = local_width // 4
    nsp = lax.axis_size("sp")
    nz = nsp // 4
    total = HALO + 4 * own
    tile_docs = jnp.broadcast_to((doc_ids + 1).astype(jnp.bfloat16)[:, None], (own, 128))
    tok = jnp.concatenate([tokens, tile_docs], axis=1)
    block = lax.axis_index("sp") % 4 + 4 * lax.axis_index("tp")
    scale = lax.dynamic_slice_in_dim(out_scale, block * width, width, 1)
    any_spec = pl.BlockSpec(memory_space=pl.ANY)
    vmem_spec = pl.BlockSpec(memory_space=pltpu.VMEM)
    bf16, f32 = jnp.bfloat16, jnp.float32
    dma = pltpu.SemaphoreType.DMA
    scratch = [
        pltpu.VMEM((2, total, local_width + 128), bf16),
        pltpu.VMEM((total, 8 * width), bf16),
        pltpu.VMEM((8, total, width), bf16),
        pltpu.VMEM((2, 8 * width, width), bf16),
        pltpu.VMEM((2, 2 * width, width), bf16),
        pltpu.VMEM((total, width), f32),
        pltpu.VMEM((16 + total, width), bf16),
        pltpu.VMEM((16 + total, 128), f32),
        pltpu.VMEM((2, total, width), bf16),
        pltpu.VMEM((total, width), bf16),
    ]
    parts = len(PARTS)
    scratch += [dma((n, nsp)) for _ in range(3) for n in (2, parts)]
    scratch += [dma((2, 4)), dma((parts, 4))]
    scratch += [dma((5,)) for _ in range(4)] + [dma((2,)), dma((5,))]
    scratch += [dma((5,)) for _ in range(4)] + [dma((2, 2)), dma((parts, 4)), dma((parts, 4))]
    return pl.pallas_call(
        functools.partial(fused_kernel, nz, own),
        out_shape=jax.ShapeDtypeStruct((own, local_width), bf16),
        in_specs=[any_spec, any_spec, any_spec, vmem_spec, vmem_spec],
        out_specs=any_spec,
        scratch_shapes=scratch,
        compiler_params=pltpu.CompilerParams(
            collective_id=0, has_side_effects=True, vmem_limit_bytes=60 * 1024 * 1024
        ),
    )(tok, in_proj, mix_proj, norm_gain, scale)


def solution(mesh):
    placed = (P("sp", "tp"), P("sp"), P(), P(None, "sp", "tp"), P(None, "sp", "tp"), P())
    body = fused_shards if mesh.shape["tp"] == 2 and mesh.shape["sp"] == 16 else shards
    return jax.shard_map(
        body, mesh=mesh, in_specs=placed, out_specs=P("sp", "tp"), check_vma=False
    )
```

```python
import functools

import jax
import jax.numpy as jnp
from jax import lax
from jax.experimental import pallas as pl
from jax.experimental.pallas import tpu as pltpu
from jax.sharding import PartitionSpec as P

D = 4096
WIN = 16
LAYERS = 2
HALO = LAYERS * WIN


epsilon = 1e-06


def from_behind(block, axis, distance):
    devices = range(lax.axis_size(axis))
    route = [(i - distance, i) for i in devices if i - distance in devices]
    return lax.ppermute(block, axis, route)


def partner_2(value, axis, stride):
    mask = 2**stride
    pairs = [(source, source ^ mask) for source in range(lax.axis_size(axis))]
    return lax.ppermute(value, axis, pairs)


def normalize(current, gain_row):
    values = current.astype(jnp.float32)
    scaled = values * lax.rsqrt(jnp.mean(values * values, axis=-1, keepdims=True) + epsilon)
    return (scaled * gain_row[None, :]).astype(jnp.bfloat16)


def pool_block(extended, ext_flags, own_flags, proj_f32, windows, local_rows):
    window_sum = jnp.zeros_like(proj_f32)
    window_count = jnp.zeros_like(proj_f32)
    for offset in range(WIN):
        begin = WIN - 1 - offset
        shifted = extended[begin : begin + local_rows]
        same_doc = ext_flags[begin : begin + local_rows] == own_flags
        taken = same_doc[:, None] & (offset < windows)[None, :]
        window_sum = window_sum + jnp.where(taken, shifted, jnp.float32(0.0))
        window_count = window_count + taken.astype(jnp.float32)
    return (window_sum / window_count - proj_f32).astype(jnp.bfloat16)


def shards(tokens, doc_ids, norm_gain, in_proj, mix_proj, out_scale):
    local_rows = tokens.shape[0]
    local_width = tokens.shape[1]
    block_width = D // 8
    blocks_here = local_width // block_width
    tp_count = lax.axis_size("tp")
    half_bit = tp_count.bit_length() - 2
    tp_index = lax.axis_index("tp")
    chan_start = tp_index * local_width
    channels = chan_start + jnp.arange(local_width, dtype=jnp.int32)
    windows = jnp.left_shift(jnp.int32(2), channels // block_width % 4)
    low_side = tp_index < tp_count // 2
    doc_flags = (doc_ids + 1).astype(jnp.bfloat16)
    in_whole, mix_whole = (
        lax.all_gather(in_proj, "sp", axis=1, tiled=True),
        lax.all_gather(mix_proj, "sp", axis=1, tiled=True),
    )
    current = tokens
    for depth_idx in range(LAYERS):
        gathered = lax.all_gather(current, "tp", axis=1, tiled=True)
        normed = normalize(gathered, norm_gain[depth_idx])
        proj_sum = jnp.dot(normed, in_whole[depth_idx], preferred_element_type=jnp.float32)
        projected = proj_sum.astype(jnp.bfloat16)
        tail_rows, tail_flags = from_behind(
            (projected[local_rows - (WIN - 1) :], doc_flags[local_rows - (WIN - 1) :]), "sp", 1
        )
        extended = jnp.concatenate([tail_rows, projected], axis=0).astype(jnp.float32)
        ext_flags = jnp.concatenate([tail_flags, doc_flags], axis=0)
        pooled = pool_block(
            extended, ext_flags, doc_flags, projected.astype(jnp.float32), windows, local_rows
        )
        partner = partner_2(pooled, "tp", half_bit)
        low_part = jnp.where(low_side, pooled, partner)
        high_part = jnp.where(low_side, partner, pooled)
        group_inputs = [
            jnp.concatenate(
                [
                    low_part[:, block_idx * block_width : (block_idx + 1) * block_width],
                    high_part[:, block_idx * block_width : (block_idx + 1) * block_width],
                ],
                axis=1,
            )
            for block_idx in range(blocks_here)
        ]
        shard_rows = mix_whole[depth_idx]
        pieces_out = []
        for add_block_idx in range(blocks_here):
            add_inputs = group_inputs[add_block_idx]
            pieces_out.append(
                jnp.dot(
                    add_inputs,
                    shard_rows[:, add_block_idx * block_width : (add_block_idx + 1) * block_width],
                    preferred_element_type=jnp.float32,
                )
            )
        grouped = jnp.concatenate(pieces_out, axis=1)
        scale_row = lax.dynamic_slice_in_dim(out_scale[depth_idx], chan_start, local_width, 0)
        current = (grouped * scale_row[None, :]).astype(jnp.bfloat16)
    return current


PARTS = ((0, 0, 4), (1, 0, 2), (1, 2, 2))

LAST_PARTS = range(1, len(PARTS))


def peer_of(g, k):
    return (g // 2 + k // 2) % 2 * 2 + (g % 2 + k % 2) % 2


def fused_kernel(
    nz, own, tok, doc_tile, in_w, mix_w, gain, scale, out,
    xt, normed, acts, w_in, w_mix, acc, proj, docs, pooled, last,
    rx_in, rx_mix, up_in, up_mix, dn_in, dn_mix, tx_in, tx_mix, rx_far,
    tiles, tile_rx, tile_tx,
    tok_rx, tok_prx, tok_tx, tok_ptx, halo, halo_tx, act_rx, act_prx, act_tx, act_ptx,
    pool_sem, out_rx, out_tx,
):
    sp = lax.axis_index("sp")
    c = lax.axis_index("tp")
    z, g = sp // 4, sp % 4
    total = HALO + 4 * own
    width = w_in.shape[2]
    k_in, k_mix = in_w.shape[1], mix_w.shape[1]
    partner = (sp, 1 - c)

    def peer(k):
        return (z * 4 + peer_of(g, k), c)

    def remote(src, dst, tx, rx, to):
        return pltpu.make_async_remote_copy(
            src_ref=src, dst_ref=dst, send_sem=tx, recv_sem=rx, device_id=to,
            device_id_type=pl.DeviceIdType.MESH,
        )

    barrier = pltpu.get_barrier_semaphore()

    def greet(to):
        pl.semaphore_signal(barrier, inc=1, device_id=to, device_id_type=pl.DeviceIdType.MESH)

    for k in (1, 2, 3):
        greet(peer(k))
    greet(partner)

    @pl.when(z > 0)
    def _():
        greet((sp - 4, c))

    @pl.when(z < nz - 1)
    def _():
        greet((sp + 4, c))

    ends = jnp.where(z > 0, 1, 0) + jnp.where(z < nz - 1, 1, 0)
    pl.semaphore_wait(barrier, 4 + ends)

    def in_piece(l, s):
        return w_in.at[l, pl.ds(s * k_in, k_in), :]

    def columns(kind, l, block):
        if kind == "in":
            return l, pl.ds(block * width, width)
        layer, first, count = PARTS[l]
        unit = width // 4
        return layer, pl.ds(block * width + first * unit, count * unit)

    def mix_piece(l, s):
        layer, cols = columns("mix", l, 0)
        return w_mix.at[layer, pl.ds(s * k_mix, k_mix), cols]

    kinds = {
        "in": (in_piece, in_w, rx_in, up_in, dn_in, tx_in),
        "mix": (mix_piece, mix_w, rx_mix, up_mix, dn_mix, tx_mix),
    }

    def given(kind, l, block):
        layer, cols = columns(kind, l, block)
        return kinds[kind][1].at[layer, :, cols]

    def own_weight(kind, l):
        piece, _, rx = kinds[kind][:3]
        return pltpu.make_async_copy(given(kind, l, g), piece(l, sp), rx.at[l, sp])

    def give_weight(kind, l, k):
        piece, _, rx, _, _, tx = kinds[kind]
        return remote(
            given(kind, l, peer_of(g, k)), piece(l, sp), tx.at[l, k], rx.at[l, sp], peer(k),
        )

    def relay(kind, l, s, up, src=None):
        piece, _, rx, up_tx, dn_tx, _ = kinds[kind]
        tx = up_tx if up else dn_tx
        to = sp + 4 if up else sp - 4
        src = piece(l, s) if src is None else src
        return remote(src, piece(l, s), tx.at[l, s], rx.at[l, s], (to, c))

    def arrived(kind, l, s):
        piece, _, rx = kinds[kind][:3]
        remote(piece(l, s), piece(l, s), rx.at[l, s], rx.at[l, s], partner).wait_recv()

    def send_relay(kind, l, s, up, src=None):
        @pl.when((z < nz - 1) if up else (z > 0))
        def _():
            relay(kind, l, s, up, src).start()

    def pump_plane(kind, l):
        if kind == "mix" or l:
            own_weight(kind, l).wait()
            send_relay(kind, l, sp, True)
            send_relay(kind, l, sp, False)
        for k in (1, 2, 3):
            s = z * 4 + peer_of(g, k)
            arrived(kind, l, s)
            send_relay(kind, l, s, True)
            send_relay(kind, l, s, False)

    def pump_far(kind, l, far, ks=range(4)):
        for k in ks:
            @pl.when(z >= far)
            def _():
                s = (z - far) * 4 + peer_of(g, k)
                arrived(kind, l, s)
                send_relay(kind, l, s, True)

            @pl.when(z + far < nz)
            def _():
                s = (z + far) * 4 + peer_of(g, k)
                arrived(kind, l, s)
                send_relay(kind, l, s, False)

    def pump_line(kind, l):
        for far in range(1, nz):
            pump_far(kind, l, far)

    def plane_piece(part, src):
        layer, cols = columns("mix", part, 0)
        return w_mix.at[layer, pl.ds(src * 4 * k_mix, 4 * k_mix), cols]

    def plane_relay(part, src, up):
        tx = up_mix if up else dn_mix
        spot, to = plane_piece(part, src), (sp + 4 if up else sp - 4, c)
        return remote(spot, spot, tx.at[part, src], rx_far.at[part, src], to)

    def send_plane(part, src, up):
        @pl.when((z < nz - 1) if up else (z > 0))
        def _():
            plane_relay(part, src, up).start()

    def pump_own_part(part):
        own_weight("mix", part).wait()
        for k in (1, 2, 3):
            arrived("mix", part, z * 4 + peer_of(g, k))
        send_plane(part, z, True)
        send_plane(part, z, False)

    def far_part(part, far, below):
        src = z - far if below else z + far
        spot = plane_piece(part, src)
        remote(spot, spot, rx_far.at[part, src], rx_far.at[part, src], partner).wait_recv()
        send_plane(part, src, below)

    def far_parts(part):
        for far in range(1, nz):
            for below in (True, False):
                @pl.when((z >= far) if below else (z + far < nz))
                def _():
                    far_part(part, far, below)

    def start_weights(kind, l):
        own_weight(kind, l).start()
        for k in (1, 2, 3):
            give_weight(kind, l, k).start()

    def rows_of(q):
        return pl.ds(HALO + q * own, own)

    halo_here = xt.at[c, pl.ds(0, HALO), :]
    tail = tok.at[pl.ds(own - HALO, HALO), :]
    halo_up = remote(tail, halo_here, halo_tx.at[0], halo.at[0], (sp + 4, c))
    halo_peer = {k: remote(halo_here, halo_here, halo_tx.at[k], halo.at[0], peer(k)) for k in (1, 2, 3)}
    halo_part = remote(halo_here, halo_here, halo_tx.at[4], halo.at[1], partner)

    own_tile = pltpu.make_async_copy(doc_tile, tiles.at[g], tile_rx.at[g])
    own_tile.start()
    tile_sent = [remote(doc_tile, tiles.at[g], tile_tx.at[k], tile_rx.at[g], peer(k)) for k in (1, 2, 3)]
    tile_up = remote(doc_tile, tiles.at[4], tile_tx.at[0], tile_rx.at[4], (sp + 4, c))
    tile_on = [remote(tiles.at[4], tiles.at[4], tile_tx.at[3 + k], tile_rx.at[4], peer(k)) for k in (1, 2, 3)]
    for copy in tile_sent:
        copy.start()

    @pl.when((z < nz - 1) & (g == 3))
    def _():
        halo_up.start()
        tile_up.start()

    for up in (True, False):
        send_relay("in", 0, sp, up, given("in", 0, g))
    start_weights("in", 0)
    tok_here = pltpu.make_async_copy(tok, xt.at[c, rows_of(g), :], tok_rx.at[0])
    tok_here.start()
    tok_sent = [remote(tok, xt.at[c, rows_of(g), :], tok_ptx.at[0], tok_prx.at[0], partner)]
    for k in (1, 2):
        tok_sent.append(
            remote(tok, xt.at[c, rows_of(g), :], tok_tx.at[k], tok_rx.at[k], peer(k))
        )
    for copy in tok_sent:
        copy.start()

    @pl.when(z == 0)
    def _():
        xt[:, 0:HALO, :] = jnp.zeros((2, HALO, xt.shape[2]), xt.dtype)

    docs[0 : 16 + HALO, :] = jnp.zeros((16 + HALO, 128), jnp.float32)
    proj[0:16, :] = jnp.zeros((16, width), proj.dtype)

    def spread(block, rx, tx, prx, ptx, sent):
        for k in (1, 2):
            spot = block(c, peer_of(g, k))
            remote(spot, spot, rx.at[k], rx.at[k], partner).wait_recv()
        for k in (1, 2):
            part = half_of(block(c, peer_of(g, k)), k)
            copy = remote(part, part, tx.at[2 + k], rx.at[2 + k], peer(3 - k))
            copy.start()
            sent.append(copy)
        for k in (1, 2):
            spot = block(c, peer_of(g, k))
            copy = remote(spot, spot, ptx.at[k], prx.at[k], partner)
            copy.start()
            sent.append(copy)

    def spread_end(block, rx, prx, ptx, sent):
        spot = block(c, peer_of(g, 3))
        for k in (1, 2):
            part = half_of(spot, k)
            remote(part, part, rx.at[2 + k], rx.at[2 + k], partner).wait_recv()
        copy = remote(spot, spot, ptx.at[3], prx.at[3], partner)
        copy.start()
        sent.append(copy)

    def from_partner(block, prx, k):
        spot = block(1 - c, peer_of(g, k))
        remote(spot, spot, prx.at[k], prx.at[k], partner).wait_recv()

    def half_of(spot, k):
        n = spot.shape[0] // 2
        return spot.at[pl.ds((k - 1) * n, n), :]

    def tok_block(side, q):
        return xt.at[side, rows_of(q), :]

    step = 16
    tile = total // 2
    chunk = 32

    def normalize_rows(l, load, start, count):
        def body(i, carry):
            r = pl.ds(pl.multiple_of(start + i * step, step), step)
            squares = jnp.zeros((step, 128), jnp.float32)
            for j in range(8):
                v = load(j, r).astype(jnp.float32)
                v = v * v
                for q in range(width // 128):
                    squares = squares + v[:, q * 128 : (q + 1) * 128]
            mean = jnp.sum(squares, axis=-1, keepdims=True) * (1.0 / (8 * width))
            factor = lax.rsqrt(mean + epsilon)
            for j in range(8):
                v = load(j, r).astype(jnp.float32) * factor
                normed[r, j * width : (j + 1) * width] = (
                    v * gain[l : l + 1, j * width : (j + 1) * width]
                ).astype(jnp.bfloat16)
            return carry

        lax.fori_loop(0, count // step, body, 0, unroll=2)

    def load_tokens(j, r):
        h = j // 4
        return xt[h, r, (j % 4) * width : (j % 4 + 1) * width]

    def load_acts(j, r):
        return acts[j, r, :]

    def add_plane(l, src, first=False):
        ks = pl.ds(pl.multiple_of(src * 4 * k_in, 4 * k_in), 4 * k_in)
        for m in range(2):
            r = slice(m * tile, (m + 1) * tile)
            y = jnp.dot(normed[r, ks], w_in[l, ks, :], preferred_element_type=jnp.float32)
            acc[r, :] = y if first else acc[r, :] + y

    def add_far(l, far):
        @pl.when(z >= far)
        def _():
            add_plane(l, z - far)

        @pl.when(z + far < nz)
        def _():
            add_plane(l, z + far)

    def store_proj():
        proj[16 : 16 + total, :] = acc[...].astype(jnp.bfloat16)

    def pool(flags):
        def body(i, carry):
            base = pl.multiple_of(i * chunk, chunk)
            ext = pl.ds(base, chunk + 16)
            d = docs[ext, :]
            same = []
            count = jnp.ones_like(d)
            for j in range(4):
                ok = jnp.where(pltpu.roll(d, 2**j, 0) == d, flags[j], 0.0)
                same.append(ok)
                count = count + ok * pltpu.roll(count, 2**j, 0)
            for q in range(width // 128):
                cols = slice(q * 128, (q + 1) * 128)
                p = proj[ext, cols].astype(jnp.float32)
                total_sum = p
                for j in range(4):
                    total_sum = total_sum + same[j] * pltpu.roll(total_sum, 2**j, 0)
                v = total_sum / count - p
                pooled[c, pl.ds(base, chunk), cols] = v[16:, :].astype(jnp.bfloat16)
            return carry

        lax.fori_loop(0, total // chunk, body, 0)

    flags = [jnp.where(g >= j, jnp.float32(1.0), jnp.float32(0.0)) for j in range(4)]

    def swap_pooled(l):
        here = pooled.at[c]
        return remote(here, here, pool_sem.at[l, 0], pool_sem.at[l, 1], partner)

    def pooled_arrived(l):
        there = pooled.at[1 - c]
        remote(there, there, pool_sem.at[l, 1], pool_sem.at[l, 1], partner).wait_recv()

    def mix(part, store):
        l, cols = columns("mix", part, 0)
        first = (g + 4 * c) * width + cols.start
        for m in range(2):
            r = slice(m * tile, (m + 1) * tile)
            y = jnp.dot(
                pooled[0, r, :], w_mix[l, 0:width, cols], preferred_element_type=jnp.float32
            )
            y = y + jnp.dot(
                pooled[1, r, :], w_mix[l, width : 2 * width, cols],
                preferred_element_type=jnp.float32,
            )
            store(r, cols, (y * scale[l : l + 1, pl.ds(pl.multiple_of(first, 128), cols.size)]).astype(jnp.bfloat16))

    def normalize_block(k):
        start = pl.multiple_of(HALO + peer_of(g, k) * own, 16)
        normalize_rows(0, load_tokens, start, own)

    pump_plane("in", 0)

    @pl.when((z > 0) & (g == 3))
    def _():
        remote(halo_here, halo_here, halo.at[0], halo.at[0], partner).wait_recv()
        halo_part.start()
        for k in (1, 2, 3):
            halo_peer[k].start()
        remote(tiles.at[4], tiles.at[4], tile_rx.at[4], tile_rx.at[4], partner).wait_recv()
        for copy in tile_on:
            copy.start()

    pump_far("in", 0, 1)
    tok_here.wait()
    from_partner(tok_block, tok_prx, 0)
    normalize_block(0)
    for far in range(2, nz - 1):
        pump_far("in", 0, far)
    spread(tok_block, tok_rx, tok_tx, tok_prx, tok_ptx, tok_sent)
    start_weights("mix", 0)
    start_weights("in", 1)
    for part in LAST_PARTS:
        start_weights("mix", part)

    @pl.when((z > 0) & (g != 3))
    def _():
        remote(halo_here, halo_here, halo.at[0], halo.at[0], partner).wait_recv()
        halo_part.start()
        remote(tiles.at[4], tiles.at[4], tile_rx.at[4], tile_rx.at[4], partner).wait_recv()

    for k in (1, 2):
        from_partner(tok_block, tok_prx, k)
        normalize_block(k)

    @pl.when(z > 0)
    def _():
        spot = xt.at[1 - c, pl.ds(0, HALO), :]
        remote(spot, spot, halo.at[1], halo.at[1], partner).wait_recv()

    normalize_rows(0, load_tokens, 0, HALO)
    spread_end(tok_block, tok_rx, tok_prx, tok_ptx, tok_sent)
    pump_plane("mix", 0)
    from_partner(tok_block, tok_prx, 3)
    normalize_block(3)
    own_tile.wait()
    for k in (1, 2, 3):
        spot = tiles.at[peer_of(g, k)]
        remote(spot, spot, tile_rx.at[peer_of(g, k)], tile_rx.at[peer_of(g, k)], partner).wait_recv()

    def doc_rows(q, lanes):
        return jnp.broadcast_to(tiles[q, lanes : lanes + 1, :], (128, 128)).T

    for q in range(4):
        for first in range(0, own, 128):
            count = min(128, own - first)
            start = 16 + HALO + q * own + first
            docs[start : start + count, :] = doc_rows(q, first // 128)[:count]

    @pl.when(z > 0)
    def _():
        lead = (own - HALO) % 128
        docs[16 : 16 + HALO, :] = doc_rows(4, (own - HALO) // 128)[lead : lead + HALO]

    own_weight("in", 0).wait()
    add_plane(0, z, True)
    for far in range(1, nz - 1):
        add_far(0, far)
    pump_far("in", 0, nz - 1)
    for far in range(1, nz - 1):
        pump_far("mix", 0, far)
    add_far(0, nz - 1)
    store_proj()
    pump_plane("in", 1)
    pool(flags)
    swap_pooled(0).start()
    pump_far("mix", 0, nz - 1)
    for part in LAST_PARTS:
        pump_own_part(part)
    pooled_arrived(0)
    mine = g + 4 * c

    def store_acts(r, cols, v):
        acts[mine, r, cols] = v

    mix(0, store_acts)
    here = acts.at[mine]
    act_sent = [remote(here, here, act_ptx.at[0], act_prx.at[0], partner)]
    for k in (1, 2):
        act_sent.append(remote(here, here, act_tx.at[k], act_rx.at[k], peer(k)))
    for copy in act_sent[1:] + act_sent[:1]:
        copy.start()

    def act_block(side, q):
        return acts.at[q + 4 * side]

    pump_far("in", 1, 1)
    for far in range(2, nz - 1):
        pump_far("in", 1, far, range(2))
    spread(act_block, act_rx, act_tx, act_prx, act_ptx, act_sent)
    for far in range(2, nz - 1):
        pump_far("in", 1, far, range(2, 4))
    spread_end(act_block, act_rx, act_prx, act_ptx, act_sent)
    for k in range(4):
        from_partner(act_block, act_prx, k)
    normalize_rows(1, load_acts, 0, total)
    add_plane(1, z, True)
    for far in range(1, nz - 1):
        add_far(1, far)

    @pl.when((z == 0) | (z == nz - 1))
    def _():
        for k in range(4):
            arrived("in", 1, (nz - 1 - z) * 4 + peer_of(g, k))
        add_plane(1, nz - 1 - z)

    store_proj()
    swap_pooled(0).wait_send()
    pool(flags)
    swap_pooled(1).start()
    def store_last(r, cols, v):
        last[r, cols] = v

    def out_copy(part, k):
        _, place = columns("mix", part, g)
        _, cols = columns("mix", part, 0)
        src = last.at[rows_of(peer_of(g, k)), cols]
        dst = out.at[:, place]
        if k == 0:
            return pltpu.make_async_copy(src, dst, out_rx.at[part, 0])
        return remote(src, dst, out_tx.at[part, k], out_rx.at[part, k], peer(k))

    inside = (z > 0) & (z < nz - 1)

    @pl.when(inside)
    def _():
        for part in LAST_PARTS:
            far_parts(part)

    for part in LAST_PARTS:
        @pl.when(jnp.logical_not(inside))
        def _():
            far_parts(part)

        if part == 1:
            pooled_arrived(1)
        mix(part, store_last)
        for k in (1, 2, 3, 0):
            out_copy(part, k).start()

    swap_pooled(1).wait_send()
    for kind in ("in", "mix"):
        for l in range(2 if kind == "in" else len(PARTS)):
            for k in (1, 2, 3):
                give_weight(kind, l, k).wait_send()
            if kind == "mix" and l:
                continue
            for src in range(nz):
                for k in range(4):
                    s = src * 4 + k

                    @pl.when((z >= src) & (z < nz - 1))
                    def _():
                        relay(kind, l, s, True).wait_send()

                    @pl.when((z <= src) & (z > 0))
                    def _():
                        relay(kind, l, s, False).wait_send()

    for part in LAST_PARTS:
        for src in range(nz):
            @pl.when((z >= src) & (z < nz - 1))
            def _():
                plane_relay(part, src, True).wait_send()

            @pl.when((z <= src) & (z > 0))
            def _():
                plane_relay(part, src, False).wait_send()

    for copy in tile_sent:
        copy.wait_send()

    @pl.when((z < nz - 1) & (g == 3))
    def _():
        halo_up.wait_send()
        tile_up.wait_send()

    @pl.when(z > 0)
    def _():
        halo_part.wait_send()

        @pl.when(g == 3)
        def _():
            for k in (1, 2, 3):
                halo_peer[k].wait_send()
            for copy in tile_on:
                copy.wait_send()

    for copy in tok_sent + act_sent:
        copy.wait_send()
    for part in LAST_PARTS:
        for k in (1, 2, 3):
            _, place = columns("mix", part, peer_of(g, k))
            _, cols = columns("mix", part, 0)
            remote(
                last.at[rows_of(peer_of(g, k)), cols], out.at[:, place],
                out_tx.at[part, k], out_rx.at[part, k], peer(k),
            ).wait()
        out_copy(part, 0).wait()


def fused_shards(tokens, doc_ids, norm_gain, in_proj, mix_proj, out_scale):
    own, local_width = tokens.shape
    width = local_width // 4
    nsp = lax.axis_size("sp")
    nz = nsp // 4
    total = HALO + 4 * own
    numbers = (doc_ids + 1).astype(jnp.float32)
    doc_tile = jnp.pad(numbers, (0, 8 * 128 - own)).reshape(8, 128)
    any_spec = pl.BlockSpec(memory_space=pl.ANY)
    vmem_spec = pl.BlockSpec(memory_space=pltpu.VMEM)
    bf16, f32 = jnp.bfloat16, jnp.float32
    dma = pltpu.SemaphoreType.DMA
    scratch = [
        pltpu.VMEM((2, total, local_width), bf16),
        pltpu.VMEM((total, 8 * width), bf16),
        pltpu.VMEM((8, total, width), bf16),
        pltpu.VMEM((2, 8 * width, width), bf16),
        pltpu.VMEM((2, 2 * width, width), bf16),
        pltpu.VMEM((total, width), f32),
        pltpu.VMEM((16 + total, width), bf16),
        pltpu.VMEM((16 + total, 128), f32),
        pltpu.VMEM((2, total, width), bf16),
        pltpu.VMEM((total, width), bf16),
    ]
    parts = len(PARTS)
    scratch += [dma((n, nsp)) for _ in range(3) for n in (2, parts)]
    scratch += [dma((2, 4)), dma((parts, 4)), dma((parts, 4))]
    scratch += [pltpu.VMEM((5, 8, 128), f32), dma((5,)), dma((7,))]
    scratch += [dma((5,)) for _ in range(4)] + [dma((2,)), dma((5,))]
    scratch += [dma((5,)) for _ in range(4)] + [dma((2, 2)), dma((parts, 4)), dma((parts, 4))]
    return pl.pallas_call(
        functools.partial(fused_kernel, nz, own),
        out_shape=jax.ShapeDtypeStruct((own, local_width), bf16),
        in_specs=[any_spec, vmem_spec, any_spec, any_spec, vmem_spec, vmem_spec],
        out_specs=any_spec,
        scratch_shapes=scratch,
        compiler_params=pltpu.CompilerParams(
            collective_id=0, has_side_effects=True, vmem_limit_bytes=60 * 1024 * 1024
        ),
    )(tokens, doc_tile, in_proj, mix_proj, norm_gain, out_scale)


def solution(mesh):
    placed = (P("sp", "tp"), P("sp"), P(), P(None, "sp", "tp"), P(None, "sp", "tp"), P())
    body = fused_shards if mesh.shape["tp"] == 2 and mesh.shape["sp"] == 16 else shards
    return jax.shard_map(
        body, mesh=mesh, in_specs=placed, out_specs=P("sp", "tp"), check_vma=False
    )
```

```python
import functools

import jax
import jax.numpy as jnp
from jax import lax
from jax.experimental import pallas as pl
from jax.experimental.pallas import tpu as pltpu
from jax.sharding import PartitionSpec as P

D = 4096
WIN = 16
LAYERS = 2
HALO = LAYERS * WIN


epsilon = 1e-06


def from_behind(block, axis, distance):
    devices = range(lax.axis_size(axis))
    route = [(i - distance, i) for i in devices if i - distance in devices]
    return lax.ppermute(block, axis, route)


def partner_2(value, axis, stride):
    mask = 2**stride
    pairs = [(source, source ^ mask) for source in range(lax.axis_size(axis))]
    return lax.ppermute(value, axis, pairs)


def normalize(current, gain_row):
    values = current.astype(jnp.float32)
    scaled = values * lax.rsqrt(jnp.mean(values * values, axis=-1, keepdims=True) + epsilon)
    return (scaled * gain_row[None, :]).astype(jnp.bfloat16)


def pool_block(extended, ext_flags, own_flags, proj_f32, windows, local_rows):
    window_sum = jnp.zeros_like(proj_f32)
    window_count = jnp.zeros_like(proj_f32)
    for offset in range(WIN):
        begin = WIN - 1 - offset
        shifted = extended[begin : begin + local_rows]
        same_doc = ext_flags[begin : begin + local_rows] == own_flags
        taken = same_doc[:, None] & (offset < windows)[None, :]
        window_sum = window_sum + jnp.where(taken, shifted, jnp.float32(0.0))
        window_count = window_count + taken.astype(jnp.float32)
    return (window_sum / window_count - proj_f32).astype(jnp.bfloat16)


def shards(tokens, doc_ids, norm_gain, in_proj, mix_proj, out_scale):
    local_rows = tokens.shape[0]
    local_width = tokens.shape[1]
    block_width = D // 8
    blocks_here = local_width // block_width
    tp_count = lax.axis_size("tp")
    half_bit = tp_count.bit_length() - 2
    tp_index = lax.axis_index("tp")
    chan_start = tp_index * local_width
    channels = chan_start + jnp.arange(local_width, dtype=jnp.int32)
    windows = jnp.left_shift(jnp.int32(2), channels // block_width % 4)
    low_side = tp_index < tp_count // 2
    doc_flags = (doc_ids + 1).astype(jnp.bfloat16)
    in_whole, mix_whole = (
        lax.all_gather(in_proj, "sp", axis=1, tiled=True),
        lax.all_gather(mix_proj, "sp", axis=1, tiled=True),
    )
    current = tokens
    for depth_idx in range(LAYERS):
        gathered = lax.all_gather(current, "tp", axis=1, tiled=True)
        normed = normalize(gathered, norm_gain[depth_idx])
        proj_sum = jnp.dot(normed, in_whole[depth_idx], preferred_element_type=jnp.float32)
        projected = proj_sum.astype(jnp.bfloat16)
        tail_rows, tail_flags = from_behind(
            (projected[local_rows - (WIN - 1) :], doc_flags[local_rows - (WIN - 1) :]), "sp", 1
        )
        extended = jnp.concatenate([tail_rows, projected], axis=0).astype(jnp.float32)
        ext_flags = jnp.concatenate([tail_flags, doc_flags], axis=0)
        pooled = pool_block(
            extended, ext_flags, doc_flags, projected.astype(jnp.float32), windows, local_rows
        )
        partner = partner_2(pooled, "tp", half_bit)
        low_part = jnp.where(low_side, pooled, partner)
        high_part = jnp.where(low_side, partner, pooled)
        group_inputs = [
            jnp.concatenate(
                [
                    low_part[:, block_idx * block_width : (block_idx + 1) * block_width],
                    high_part[:, block_idx * block_width : (block_idx + 1) * block_width],
                ],
                axis=1,
            )
            for block_idx in range(blocks_here)
        ]
        shard_rows = mix_whole[depth_idx]
        pieces_out = []
        for add_block_idx in range(blocks_here):
            add_inputs = group_inputs[add_block_idx]
            pieces_out.append(
                jnp.dot(
                    add_inputs,
                    shard_rows[:, add_block_idx * block_width : (add_block_idx + 1) * block_width],
                    preferred_element_type=jnp.float32,
                )
            )
        grouped = jnp.concatenate(pieces_out, axis=1)
        scale_row = lax.dynamic_slice_in_dim(out_scale[depth_idx], chan_start, local_width, 0)
        current = (grouped * scale_row[None, :]).astype(jnp.bfloat16)
    return current


PARTS = ((0, 0, 4), (1, 0, 2), (1, 2, 2))

LAST_PARTS = range(1, len(PARTS))


def peer_of(g, k):
    return (g // 2 + k // 2) % 2 * 2 + (g % 2 + k % 2) % 2


def fused_kernel(
    nz, own, tok, doc_tile, in_w, mix_w, gain, scale, out,
    xt, normed, acts, w_in, w_mix, acc, proj, docs, pooled, last,
    rx_in, rx_mix, up_in, up_mix, dn_in, dn_mix, tx_in, tx_mix, rx_far,
    tiles, tile_rx, tile_tx,
    tok_rx, tok_prx, tok_tx, tok_ptx, halo, halo_tx, act_rx, act_prx, act_tx, act_ptx,
    pool_sem, out_rx, out_tx,
):
    sp = lax.axis_index("sp")
    c = lax.axis_index("tp")
    z, g = sp // 4, sp % 4
    total = HALO + 4 * own
    width = w_in.shape[2]
    k_in, k_mix = in_w.shape[1], mix_w.shape[1]
    partner = (sp, 1 - c)

    def peer(k):
        return (z * 4 + peer_of(g, k), c)

    def remote(src, dst, tx, rx, to):
        return pltpu.make_async_remote_copy(
            src_ref=src, dst_ref=dst, send_sem=tx, recv_sem=rx, device_id=to,
            device_id_type=pl.DeviceIdType.MESH,
        )

    barrier = pltpu.get_barrier_semaphore()

    def greet(to):
        pl.semaphore_signal(barrier, inc=1, device_id=to, device_id_type=pl.DeviceIdType.MESH)

    for k in (1, 2, 3):
        greet(peer(k))
    greet(partner)

    @pl.when(z > 0)
    def _():
        greet((sp - 4, c))

    @pl.when(z < nz - 1)
    def _():
        greet((sp + 4, c))

    ends = jnp.where(z > 0, 1, 0) + jnp.where(z < nz - 1, 1, 0)
    pl.semaphore_wait(barrier, 4 + ends)

    def in_piece(l, s):
        return w_in.at[l, pl.ds(s * k_in, k_in), :]

    def columns(kind, l, block):
        if kind == "in":
            return l, pl.ds(block * width, width)
        layer, first, count = PARTS[l]
        unit = width // 4
        return layer, pl.ds(block * width + first * unit, count * unit)

    def mix_piece(l, s):
        layer, cols = columns("mix", l, 0)
        return w_mix.at[layer, pl.ds(s * k_mix, k_mix), cols]

    kinds = {
        "in": (in_piece, in_w, rx_in, up_in, dn_in, tx_in),
        "mix": (mix_piece, mix_w, rx_mix, up_mix, dn_mix, tx_mix),
    }

    def given(kind, l, block):
        layer, cols = columns(kind, l, block)
        return kinds[kind][1].at[layer, :, cols]

    def own_weight(kind, l):
        piece, _, rx = kinds[kind][:3]
        return pltpu.make_async_copy(given(kind, l, g), piece(l, sp), rx.at[l, sp])

    def give_weight(kind, l, k):
        piece, _, rx, _, _, tx = kinds[kind]
        return remote(
            given(kind, l, peer_of(g, k)), piece(l, sp), tx.at[l, k], rx.at[l, sp], peer(k),
        )

    def relay(kind, l, s, up, src=None):
        piece, _, rx, up_tx, dn_tx, _ = kinds[kind]
        tx = up_tx if up else dn_tx
        to = sp + 4 if up else sp - 4
        src = piece(l, s) if src is None else src
        return remote(src, piece(l, s), tx.at[l, s], rx.at[l, s], (to, c))

    def arrived(kind, l, s):
        piece, _, rx = kinds[kind][:3]
        remote(piece(l, s), piece(l, s), rx.at[l, s], rx.at[l, s], partner).wait_recv()

    def send_relay(kind, l, s, up, src=None):
        @pl.when((z < nz - 1) if up else (z > 0))
        def _():
            relay(kind, l, s, up, src).start()

    def pump_plane(kind, l):
        if kind == "mix" or l:
            own_weight(kind, l).wait()
            send_relay(kind, l, sp, True)
            send_relay(kind, l, sp, False)
        for k in (1, 2, 3):
            s = z * 4 + peer_of(g, k)
            arrived(kind, l, s)
            send_relay(kind, l, s, True)
            send_relay(kind, l, s, False)

    def pump_far(kind, l, far, ks=range(4)):
        for k in ks:
            @pl.when(z >= far)
            def _():
                s = (z - far) * 4 + peer_of(g, k)
                arrived(kind, l, s)
                send_relay(kind, l, s, True)

            @pl.when(z + far < nz)
            def _():
                s = (z + far) * 4 + peer_of(g, k)
                arrived(kind, l, s)
                send_relay(kind, l, s, False)

    def pump_line(kind, l):
        for far in range(1, nz):
            pump_far(kind, l, far)

    def plane_piece(part, src):
        layer, cols = columns("mix", part, 0)
        return w_mix.at[layer, pl.ds(src * 4 * k_mix, 4 * k_mix), cols]

    def plane_relay(part, src, up):
        tx = up_mix if up else dn_mix
        spot, to = plane_piece(part, src), (sp + 4 if up else sp - 4, c)
        return remote(spot, spot, tx.at[part, src], rx_far.at[part, src], to)

    def send_plane(part, src, up):
        @pl.when((z < nz - 1) if up else (z > 0))
        def _():
            plane_relay(part, src, up).start()

    def pump_own_part(part):
        own_weight("mix", part).wait()
        for k in (1, 2, 3):
            arrived("mix", part, z * 4 + peer_of(g, k))
        send_plane(part, z, True)
        send_plane(part, z, False)

    def far_part(part, far, below):
        src = z - far if below else z + far
        spot = plane_piece(part, src)
        remote(spot, spot, rx_far.at[part, src], rx_far.at[part, src], partner).wait_recv()
        send_plane(part, src, below)

    def far_parts(part):
        for far in range(1, nz):
            for below in (True, False):
                @pl.when((z >= far) if below else (z + far < nz))
                def _():
                    far_part(part, far, below)

    def start_weights(kind, l):
        own_weight(kind, l).start()
        for k in (1, 2, 3):
            give_weight(kind, l, k).start()

    def rows_of(q):
        return pl.ds(HALO + q * own, own)

    halo_here = xt.at[c, pl.ds(0, HALO), :]
    tail = tok.at[pl.ds(own - HALO, HALO), :]
    halo_up = remote(tail, halo_here, halo_tx.at[0], halo.at[0], (sp + 4, c))
    halo_peer = {k: remote(halo_here, halo_here, halo_tx.at[k], halo.at[0], peer(k)) for k in (1, 2, 3)}
    halo_part = remote(halo_here, halo_here, halo_tx.at[4], halo.at[1], partner)

    own_tile = pltpu.make_async_copy(doc_tile, tiles.at[g], tile_rx.at[g])
    own_tile.start()
    tile_sent = [remote(doc_tile, tiles.at[g], tile_tx.at[k], tile_rx.at[g], peer(k)) for k in (1, 2, 3)]
    tile_up = remote(doc_tile, tiles.at[4], tile_tx.at[0], tile_rx.at[4], (sp + 4, c))
    tile_on = [remote(tiles.at[4], tiles.at[4], tile_tx.at[3 + k], tile_rx.at[4], peer(k)) for k in (1, 2, 3)]
    for copy in tile_sent:
        copy.start()

    @pl.when((z < nz - 1) & (g == 3))
    def _():
        halo_up.start()
        tile_up.start()

    for up in (True, False):
        send_relay("in", 0, sp, up, given("in", 0, g))
    start_weights("in", 0)
    start_weights("mix", 0)
    tok_here = pltpu.make_async_copy(tok, xt.at[c, rows_of(g), :], tok_rx.at[0])
    tok_here.start()
    tok_sent = [remote(tok, xt.at[c, rows_of(g), :], tok_ptx.at[0], tok_prx.at[0], partner)]
    for k in (1, 2):
        tok_sent.append(
            remote(tok, xt.at[c, rows_of(g), :], tok_tx.at[k], tok_rx.at[k], peer(k))
        )
    for copy in tok_sent:
        copy.start()

    @pl.when(z == 0)
    def _():
        xt[:, 0:HALO, :] = jnp.zeros((2, HALO, xt.shape[2]), xt.dtype)

    docs[0 : 16 + HALO, :] = jnp.zeros((16 + HALO, 128), jnp.float32)
    proj[0:16, :] = jnp.zeros((16, width), proj.dtype)

    def spread(block, rx, tx, prx, ptx, sent):
        for k in (1, 2):
            spot = block(c, peer_of(g, k))
            remote(spot, spot, rx.at[k], rx.at[k], partner).wait_recv()
        for k in (1, 2):
            part = half_of(block(c, peer_of(g, k)), k)
            copy = remote(part, part, tx.at[2 + k], rx.at[2 + k], peer(3 - k))
            copy.start()
            sent.append(copy)
        for k in (1, 2):
            spot = block(c, peer_of(g, k))
            copy = remote(spot, spot, ptx.at[k], prx.at[k], partner)
            copy.start()
            sent.append(copy)

    def spread_end(block, rx, prx, ptx, sent):
        spot = block(c, peer_of(g, 3))
        for k in (1, 2):
            part = half_of(spot, k)
            remote(part, part, rx.at[2 + k], rx.at[2 + k], partner).wait_recv()
        copy = remote(spot, spot, ptx.at[3], prx.at[3], partner)
        copy.start()
        sent.append(copy)

    def from_partner(block, prx, k):
        spot = block(1 - c, peer_of(g, k))
        remote(spot, spot, prx.at[k], prx.at[k], partner).wait_recv()

    def half_of(spot, k):
        n = spot.shape[0] // 2
        return spot.at[pl.ds((k - 1) * n, n), :]

    def tok_block(side, q):
        return xt.at[side, rows_of(q), :]

    step = 16
    tile = total // 2
    chunk = 32

    def normalize_rows(l, load, start, count):
        def body(i, carry):
            r = pl.ds(pl.multiple_of(start + i * step, step), step)
            squares = jnp.zeros((step, 128), jnp.float32)
            for j in range(8):
                v = load(j, r).astype(jnp.float32)
                v = v * v
                for q in range(width // 128):
                    squares = squares + v[:, q * 128 : (q + 1) * 128]
            mean = jnp.sum(squares, axis=-1, keepdims=True) * (1.0 / (8 * width))
            factor = lax.rsqrt(mean + epsilon)
            for j in range(8):
                v = load(j, r).astype(jnp.float32) * factor
                normed[r, j * width : (j + 1) * width] = (
                    v * gain[l : l + 1, j * width : (j + 1) * width]
                ).astype(jnp.bfloat16)
            return carry

        lax.fori_loop(0, count // step, body, 0, unroll=2)

    def load_tokens(j, r):
        h = j // 4
        return xt[h, r, (j % 4) * width : (j % 4 + 1) * width]

    def load_acts(j, r):
        return acts[j, r, :]

    def add_plane(l, src, first=False):
        ks = pl.ds(pl.multiple_of(src * 4 * k_in, 4 * k_in), 4 * k_in)
        for m in range(2):
            r = slice(m * tile, (m + 1) * tile)
            y = jnp.dot(normed[r, ks], w_in[l, ks, :], preferred_element_type=jnp.float32)
            acc[r, :] = y if first else acc[r, :] + y

    def add_last(l):
        @pl.when((z == 0) | (z == nz - 1))
        def _():
            src = nz - 1 - z
            ks = pl.ds(pl.multiple_of(src * 4 * k_in, 4 * k_in), 4 * k_in)
            for m in range(2):
                r = slice(m * tile, (m + 1) * tile)
                y = jnp.dot(normed[r, ks], w_in[l, ks, :], preferred_element_type=jnp.float32)
                proj[16 + m * tile : 16 + (m + 1) * tile, :] = (acc[r, :] + y).astype(jnp.bfloat16)

        @pl.when((z > 0) & (z < nz - 1))
        def _():
            store_proj()

    def add_far(l, far):
        @pl.when(z >= far)
        def _():
            add_plane(l, z - far)

        @pl.when(z + far < nz)
        def _():
            add_plane(l, z + far)

    def store_proj():
        proj[16 : 16 + total, :] = acc[...].astype(jnp.bfloat16)

    split = total // 2 // chunk * chunk + chunk
    spans = ((0, split), (split, total - split))

    def pool(flags, first, count):
        def body(i, carry):
            base = pl.multiple_of(first + i * chunk, chunk)
            ext = pl.ds(base, chunk + 16)
            d = docs[ext, :]
            same = []
            tally = jnp.ones_like(d)
            for j in range(4):
                ok = jnp.where(pltpu.roll(d, 2**j, 0) == d, flags[j], 0.0)
                same.append(ok)
                tally = tally + ok * pltpu.roll(tally, 2**j, 0)
            share = 1.0 / tally
            for q in range(width // 128):
                cols = slice(q * 128, (q + 1) * 128)
                p = proj[ext, cols].astype(jnp.float32)
                total_sum = p
                for j in range(4):
                    total_sum = total_sum + same[j] * pltpu.roll(total_sum, 2**j, 0)
                v = total_sum * share - p
                pooled[c, pl.ds(base, chunk), cols] = v[16:, :].astype(jnp.bfloat16)
            return carry

        lax.fori_loop(0, count // chunk, body, 0)

    flags = [jnp.where(g >= j, jnp.float32(1.0), jnp.float32(0.0)) for j in range(4)]

    def swap_pooled(l, h):
        here = pooled.at[c, pl.ds(*spans[h]), :]
        return remote(here, here, pool_sem.at[l, h], pool_sem.at[l, 2 + h], partner)

    def pooled_arrived(l, h):
        there = pooled.at[1 - c, pl.ds(*spans[h]), :]
        remote(there, there, pool_sem.at[l, 2 + h], pool_sem.at[l, 2 + h], partner).wait_recv()

    def pool_and_swap(l):
        for h in range(2):
            pool(flags, *spans[h])
            swap_pooled(l, h).start()

    def mix(part, spans, store):
        l, cols = columns("mix", part, 0)
        first = (g + 4 * c) * width + cols.start
        for r in spans:
            y = jnp.dot(
                pooled[0, r, :], w_mix[l, 0:width, cols], preferred_element_type=jnp.float32
            )
            y = y + jnp.dot(
                pooled[1, r, :], w_mix[l, width : 2 * width, cols],
                preferred_element_type=jnp.float32,
            )
            store(r, cols, (y * scale[l : l + 1, pl.ds(pl.multiple_of(first, 128), cols.size)]).astype(jnp.bfloat16))

    def normalize_block(k):
        start = pl.multiple_of(HALO + peer_of(g, k) * own, 16)
        normalize_rows(0, load_tokens, start, own)

    pump_plane("in", 0)
    pump_plane("mix", 0)

    @pl.when((z > 0) & (g == 3))
    def _():
        remote(halo_here, halo_here, halo.at[0], halo.at[0], partner).wait_recv()
        halo_part.start()
        for k in (1, 2, 3):
            halo_peer[k].start()
        remote(tiles.at[4], tiles.at[4], tile_rx.at[4], tile_rx.at[4], partner).wait_recv()
        for copy in tile_on:
            copy.start()

    pump_far("in", 0, 1)
    pump_far("mix", 0, 1)
    tok_here.wait()
    from_partner(tok_block, tok_prx, 0)
    normalize_block(0)
    for far in range(2, nz - 1):
        pump_far("in", 0, far)
        pump_far("mix", 0, far)
    spread(tok_block, tok_rx, tok_tx, tok_prx, tok_ptx, tok_sent)
    start_weights("in", 1)
    for part in LAST_PARTS:
        start_weights("mix", part)

    @pl.when((z > 0) & (g != 3))
    def _():
        remote(halo_here, halo_here, halo.at[0], halo.at[0], partner).wait_recv()
        halo_part.start()
        remote(tiles.at[4], tiles.at[4], tile_rx.at[4], tile_rx.at[4], partner).wait_recv()

    for k in (1, 2):
        from_partner(tok_block, tok_prx, k)
        normalize_block(k)

    @pl.when(z > 0)
    def _():
        spot = xt.at[1 - c, pl.ds(0, HALO), :]
        remote(spot, spot, halo.at[1], halo.at[1], partner).wait_recv()

    normalize_rows(0, load_tokens, 0, HALO)
    spread_end(tok_block, tok_rx, tok_prx, tok_ptx, tok_sent)
    from_partner(tok_block, tok_prx, 3)
    normalize_block(3)
    own_tile.wait()
    for k in (1, 2, 3):
        spot = tiles.at[peer_of(g, k)]
        remote(spot, spot, tile_rx.at[peer_of(g, k)], tile_rx.at[peer_of(g, k)], partner).wait_recv()

    def doc_rows(q, lanes):
        return jnp.broadcast_to(tiles[q, lanes : lanes + 1, :], (128, 128)).T

    for q in range(4):
        for first in range(0, own, 128):
            count = min(128, own - first)
            start = 16 + HALO + q * own + first
            docs[start : start + count, :] = doc_rows(q, first // 128)[:count]

    @pl.when(z > 0)
    def _():
        lead = (own - HALO) % 128
        docs[16 : 16 + HALO, :] = doc_rows(4, (own - HALO) // 128)[lead : lead + HALO]

    own_weight("in", 0).wait()
    add_plane(0, z, True)
    for far in range(1, nz - 1):
        add_far(0, far)
    pump_far("in", 0, nz - 1)
    add_last(0)
    pump_plane("in", 1)
    pool_and_swap(0)
    pump_far("mix", 0, nz - 1)
    inside = (z > 0) & (z < nz - 1)

    @pl.when(jnp.logical_not(inside))
    def _():
        for part in LAST_PARTS:
            pump_own_part(part)

    for h in range(2):
        pooled_arrived(0, h)
    mine = g + 4 * c

    def store_acts(r, cols, v):
        acts[mine, r, cols] = v

    mix(0, [slice(m * tile, (m + 1) * tile) for m in range(2)], store_acts)
    here = acts.at[mine]
    act_sent = [remote(here, here, act_ptx.at[0], act_prx.at[0], partner)]
    for k in (1, 2):
        act_sent.append(remote(here, here, act_tx.at[k], act_rx.at[k], peer(k)))
    for copy in act_sent[1:] + act_sent[:1]:
        copy.start()

    def act_block(side, q):
        return acts.at[q + 4 * side]

    pump_far("in", 1, 1)
    for far in range(2, nz - 1):
        pump_far("in", 1, far, range(2))
    spread(act_block, act_rx, act_tx, act_prx, act_ptx, act_sent)
    for far in range(2, nz - 1):
        pump_far("in", 1, far, range(2, 4))
    spread_end(act_block, act_rx, act_prx, act_ptx, act_sent)

    @pl.when(inside)
    def _():
        for part in LAST_PARTS:
            pump_own_part(part)

    for k in range(4):
        from_partner(act_block, act_prx, k)
    normalize_rows(1, load_acts, 0, total)
    add_plane(1, z, True)
    for far in range(1, nz - 1):
        add_far(1, far)

    @pl.when((z == 0) | (z == nz - 1))
    def _():
        for k in range(4):
            arrived("in", 1, (nz - 1 - z) * 4 + peer_of(g, k))

    add_last(1)
    for h in range(2):
        swap_pooled(0, h).wait_send()
    pool_and_swap(1)
    @pl.when(inside)
    def _():
        for part in LAST_PARTS:
            far_parts(part)

    def store_last(r, cols, v):
        last[r, cols] = v

    def out_copy(part, k):
        _, place = columns("mix", part, g)
        _, cols = columns("mix", part, 0)
        src = last.at[rows_of(peer_of(g, k)), cols]
        dst = out.at[:, place]
        if k == 0:
            return pltpu.make_async_copy(src, dst, out_rx.at[part, 0])
        return remote(src, dst, out_tx.at[part, k], out_rx.at[part, k], peer(k))

    for part in LAST_PARTS:
        @pl.when(jnp.logical_not(inside))
        def _():
            far_parts(part)

        if part == 1:
            for h in range(2):
                pooled_arrived(1, h)
        for k in (3, 1, 2, 0):
            start = pl.multiple_of(HALO + peer_of(g, k) * own, 16)
            mix(part, [pl.ds(start, own)], store_last)
            out_copy(part, k).start()

    for h in range(2):
        swap_pooled(1, h).wait_send()
    for kind in ("in", "mix"):
        for l in range(2 if kind == "in" else len(PARTS)):
            for k in (1, 2, 3):
                give_weight(kind, l, k).wait_send()
            if kind == "mix" and l:
                continue
            for src in range(nz):
                for k in range(4):
                    s = src * 4 + k

                    @pl.when((z >= src) & (z < nz - 1))
                    def _():
                        relay(kind, l, s, True).wait_send()

                    @pl.when((z <= src) & (z > 0))
                    def _():
                        relay(kind, l, s, False).wait_send()

    for part in LAST_PARTS:
        for src in range(nz):
            @pl.when((z >= src) & (z < nz - 1))
            def _():
                plane_relay(part, src, True).wait_send()

            @pl.when((z <= src) & (z > 0))
            def _():
                plane_relay(part, src, False).wait_send()

    for copy in tile_sent:
        copy.wait_send()

    @pl.when((z < nz - 1) & (g == 3))
    def _():
        halo_up.wait_send()
        tile_up.wait_send()

    @pl.when(z > 0)
    def _():
        halo_part.wait_send()

        @pl.when(g == 3)
        def _():
            for k in (1, 2, 3):
                halo_peer[k].wait_send()
            for copy in tile_on:
                copy.wait_send()

    for copy in tok_sent + act_sent:
        copy.wait_send()
    for part in LAST_PARTS:
        for k in (1, 2, 3):
            _, place = columns("mix", part, peer_of(g, k))
            _, cols = columns("mix", part, 0)
            remote(
                last.at[rows_of(peer_of(g, k)), cols], out.at[:, place],
                out_tx.at[part, k], out_rx.at[part, k], peer(k),
            ).wait()
        out_copy(part, 0).wait()


def fused_shards(tokens, doc_ids, norm_gain, in_proj, mix_proj, out_scale):
    own, local_width = tokens.shape
    width = local_width // 4
    nsp = lax.axis_size("sp")
    nz = nsp // 4
    total = HALO + 4 * own
    numbers = (doc_ids + 1).astype(jnp.float32)
    doc_tile = jnp.pad(numbers, (0, 8 * 128 - own)).reshape(8, 128)
    any_spec = pl.BlockSpec(memory_space=pl.ANY)
    vmem_spec = pl.BlockSpec(memory_space=pltpu.VMEM)
    bf16, f32 = jnp.bfloat16, jnp.float32
    dma = pltpu.SemaphoreType.DMA
    scratch = [
        pltpu.VMEM((2, total, local_width), bf16),
        pltpu.VMEM((total, 8 * width), bf16),
        pltpu.VMEM((8, total, width), bf16),
        pltpu.VMEM((2, 8 * width, width), bf16),
        pltpu.VMEM((2, 2 * width, width), bf16),
        pltpu.VMEM((total, width), f32),
        pltpu.VMEM((16 + total, width), bf16),
        pltpu.VMEM((16 + total, 128), f32),
        pltpu.VMEM((2, total, width), bf16),
        pltpu.VMEM((total, width), bf16),
    ]
    parts = len(PARTS)
    scratch += [dma((n, nsp)) for _ in range(3) for n in (2, parts)]
    scratch += [dma((2, 4)), dma((parts, 4)), dma((parts, 4))]
    scratch += [pltpu.VMEM((5, 8, 128), f32), dma((5,)), dma((7,))]
    scratch += [dma((5,)) for _ in range(4)] + [dma((2,)), dma((5,))]
    scratch += [dma((5,)) for _ in range(4)] + [dma((2, 4)), dma((parts, 4)), dma((parts, 4))]
    return pl.pallas_call(
        functools.partial(fused_kernel, nz, own),
        out_shape=jax.ShapeDtypeStruct((own, local_width), bf16),
        in_specs=[any_spec, vmem_spec, any_spec, any_spec, vmem_spec, vmem_spec],
        out_specs=any_spec,
        scratch_shapes=scratch,
        compiler_params=pltpu.CompilerParams(
            collective_id=0, has_side_effects=True, vmem_limit_bytes=60 * 1024 * 1024
        ),
    )(tokens, doc_tile, in_proj, mix_proj, norm_gain, out_scale)


def solution(mesh):
    placed = (P("sp", "tp"), P("sp"), P(), P(None, "sp", "tp"), P(None, "sp", "tp"), P())
    body = fused_shards if mesh.shape["tp"] == 2 and mesh.shape["sp"] == 16 else shards
    return jax.shard_map(
        body, mesh=mesh, in_specs=placed, out_specs=P("sp", "tp"), check_vma=False
    )
```

```python
import functools

import jax
import jax.numpy as jnp
from jax import lax
from jax.experimental import pallas as pl
from jax.experimental.pallas import tpu as pltpu
from jax.sharding import PartitionSpec as P

D = 4096
WIN = 16
LAYERS = 2
HALO = LAYERS * WIN


epsilon = 1e-06


def from_behind(block, axis, distance):
    devices = range(lax.axis_size(axis))
    route = [(i - distance, i) for i in devices if i - distance in devices]
    return lax.ppermute(block, axis, route)


def partner_2(value, axis, stride):
    mask = 2**stride
    pairs = [(source, source ^ mask) for source in range(lax.axis_size(axis))]
    return lax.ppermute(value, axis, pairs)


def normalize(current, gain_row):
    values = current.astype(jnp.float32)
    scaled = values * lax.rsqrt(jnp.mean(values * values, axis=-1, keepdims=True) + epsilon)
    return (scaled * gain_row[None, :]).astype(jnp.bfloat16)


def pool_block(extended, ext_flags, own_flags, proj_f32, windows, local_rows):
    window_sum = jnp.zeros_like(proj_f32)
    window_count = jnp.zeros_like(proj_f32)
    for offset in range(WIN):
        begin = WIN - 1 - offset
        shifted = extended[begin : begin + local_rows]
        same_doc = ext_flags[begin : begin + local_rows] == own_flags
        taken = same_doc[:, None] & (offset < windows)[None, :]
        window_sum = window_sum + jnp.where(taken, shifted, jnp.float32(0.0))
        window_count = window_count + taken.astype(jnp.float32)
    return (window_sum / window_count - proj_f32).astype(jnp.bfloat16)


def shards(tokens, doc_ids, norm_gain, in_proj, mix_proj, out_scale):
    local_rows = tokens.shape[0]
    local_width = tokens.shape[1]
    block_width = D // 8
    blocks_here = local_width // block_width
    tp_count = lax.axis_size("tp")
    half_bit = tp_count.bit_length() - 2
    tp_index = lax.axis_index("tp")
    chan_start = tp_index * local_width
    channels = chan_start + jnp.arange(local_width, dtype=jnp.int32)
    windows = jnp.left_shift(jnp.int32(2), channels // block_width % 4)
    low_side = tp_index < tp_count // 2
    doc_flags = (doc_ids + 1).astype(jnp.bfloat16)
    in_whole, mix_whole = (
        lax.all_gather(in_proj, "sp", axis=1, tiled=True),
        lax.all_gather(mix_proj, "sp", axis=1, tiled=True),
    )
    current = tokens
    for depth_idx in range(LAYERS):
        gathered = lax.all_gather(current, "tp", axis=1, tiled=True)
        normed = normalize(gathered, norm_gain[depth_idx])
        proj_sum = jnp.dot(normed, in_whole[depth_idx], preferred_element_type=jnp.float32)
        projected = proj_sum.astype(jnp.bfloat16)
        tail_rows, tail_flags = from_behind(
            (projected[local_rows - (WIN - 1) :], doc_flags[local_rows - (WIN - 1) :]), "sp", 1
        )
        extended = jnp.concatenate([tail_rows, projected], axis=0).astype(jnp.float32)
        ext_flags = jnp.concatenate([tail_flags, doc_flags], axis=0)
        pooled = pool_block(
            extended, ext_flags, doc_flags, projected.astype(jnp.float32), windows, local_rows
        )
        partner = partner_2(pooled, "tp", half_bit)
        low_part = jnp.where(low_side, pooled, partner)
        high_part = jnp.where(low_side, partner, pooled)
        group_inputs = [
            jnp.concatenate(
                [
                    low_part[:, block_idx * block_width : (block_idx + 1) * block_width],
                    high_part[:, block_idx * block_width : (block_idx + 1) * block_width],
                ],
                axis=1,
            )
            for block_idx in range(blocks_here)
        ]
        shard_rows = mix_whole[depth_idx]
        pieces_out = []
        for add_block_idx in range(blocks_here):
            add_inputs = group_inputs[add_block_idx]
            pieces_out.append(
                jnp.dot(
                    add_inputs,
                    shard_rows[:, add_block_idx * block_width : (add_block_idx + 1) * block_width],
                    preferred_element_type=jnp.float32,
                )
            )
        grouped = jnp.concatenate(pieces_out, axis=1)
        scale_row = lax.dynamic_slice_in_dim(out_scale[depth_idx], chan_start, local_width, 0)
        current = (grouped * scale_row[None, :]).astype(jnp.bfloat16)
    return current


PARTS = ((0, 0, 4), (1, 0, 2), (1, 2, 2))

LAST_PARTS = range(1, len(PARTS))


def peer_of(g, k):
    return (g // 2 + k // 2) % 2 * 2 + (g % 2 + k % 2) % 2


def fused_kernel(
    nz, own, tok, doc_tile, in_w, mix_w, gain, scale, out,
    xt, normed, acts, w_in, w_mix, acc, proj, docs, pooled, last,
    rx_in, rx_mix, up_in, up_mix, dn_in, dn_mix, tx_in, tx_mix, rx_far,
    tiles, tile_rx, tile_tx,
    tok_rx, tok_prx, tok_tx, tok_ptx, halo, halo_tx, act_rx, act_prx, act_tx, act_ptx,
    pool_sem, out_rx, out_tx,
):
    sp = lax.axis_index("sp")
    c = lax.axis_index("tp")
    z, g = sp // 4, sp % 4
    total = HALO + 4 * own
    width = w_in.shape[2]
    k_in, k_mix = in_w.shape[1], mix_w.shape[1]
    partner = (sp, 1 - c)

    def peer(k):
        return (z * 4 + peer_of(g, k), c)

    def remote(src, dst, tx, rx, to):
        return pltpu.make_async_remote_copy(
            src_ref=src, dst_ref=dst, send_sem=tx, recv_sem=rx, device_id=to,
            device_id_type=pl.DeviceIdType.MESH,
        )

    barrier = pltpu.get_barrier_semaphore()

    def greet(to):
        pl.semaphore_signal(barrier, inc=1, device_id=to, device_id_type=pl.DeviceIdType.MESH)

    for k in (1, 2, 3):
        greet(peer(k))
    greet(partner)

    @pl.when(z > 0)
    def _():
        greet((sp - 4, c))

    @pl.when(z < nz - 1)
    def _():
        greet((sp + 4, c))

    ends = jnp.where(z > 0, 1, 0) + jnp.where(z < nz - 1, 1, 0)
    pl.semaphore_wait(barrier, 4 + ends)

    def in_piece(l, s):
        return w_in.at[l, pl.ds(s * k_in, k_in), :]

    def columns(kind, l, block):
        if kind == "in":
            return l, pl.ds(block * width, width)
        layer, first, count = PARTS[l]
        unit = width // 4
        return layer, pl.ds(block * width + first * unit, count * unit)

    def mix_piece(l, s):
        layer, cols = columns("mix", l, 0)
        return w_mix.at[layer, pl.ds(s * k_mix, k_mix), cols]

    kinds = {
        "in": (in_piece, in_w, rx_in, up_in, dn_in, tx_in),
        "mix": (mix_piece, mix_w, rx_mix, up_mix, dn_mix, tx_mix),
    }

    def given(kind, l, block):
        layer, cols = columns(kind, l, block)
        return kinds[kind][1].at[layer, :, cols]

    def own_weight(kind, l):
        piece, _, rx = kinds[kind][:3]
        return pltpu.make_async_copy(given(kind, l, g), piece(l, sp), rx.at[l, sp])

    def give_weight(kind, l, k):
        piece, _, rx, _, _, tx = kinds[kind]
        return remote(
            given(kind, l, peer_of(g, k)), piece(l, sp), tx.at[l, k], rx.at[l, sp], peer(k),
        )

    def relay(kind, l, s, up, src=None):
        piece, _, rx, up_tx, dn_tx, _ = kinds[kind]
        tx = up_tx if up else dn_tx
        to = sp + 4 if up else sp - 4
        src = piece(l, s) if src is None else src
        return remote(src, piece(l, s), tx.at[l, s], rx.at[l, s], (to, c))

    def arrived(kind, l, s):
        piece, _, rx = kinds[kind][:3]
        remote(piece(l, s), piece(l, s), rx.at[l, s], rx.at[l, s], partner).wait_recv()

    def send_relay(kind, l, s, up, src=None):
        @pl.when((z < nz - 1) if up else (z > 0))
        def _():
            relay(kind, l, s, up, src).start()

    def pump_plane(kind, l):
        if kind == "mix" or l:
            own_weight(kind, l).wait()
            send_relay(kind, l, sp, True)
            send_relay(kind, l, sp, False)
        for k in (1, 2, 3):
            s = z * 4 + peer_of(g, k)
            arrived(kind, l, s)
            send_relay(kind, l, s, True)
            send_relay(kind, l, s, False)

    def pump_far(kind, l, far, ks=range(4)):
        for k in ks:
            @pl.when(z >= far)
            def _():
                s = (z - far) * 4 + peer_of(g, k)
                arrived(kind, l, s)
                send_relay(kind, l, s, True)

            @pl.when(z + far < nz)
            def _():
                s = (z + far) * 4 + peer_of(g, k)
                arrived(kind, l, s)
                send_relay(kind, l, s, False)

    def pump_line(kind, l):
        for far in range(1, nz):
            pump_far(kind, l, far)

    def plane_piece(part, src):
        layer, cols = columns("mix", part, 0)
        return w_mix.at[layer, pl.ds(src * 4 * k_mix, 4 * k_mix), cols]

    def plane_relay(part, src, up):
        tx = up_mix if up else dn_mix
        spot, to = plane_piece(part, src), (sp + 4 if up else sp - 4, c)
        return remote(spot, spot, tx.at[part, src], rx_far.at[part, src], to)

    def send_plane(part, src, up):
        @pl.when((z < nz - 1) if up else (z > 0))
        def _():
            plane_relay(part, src, up).start()

    def pump_own_part(part):
        own_weight("mix", part).wait()
        for k in (1, 2, 3):
            arrived("mix", part, z * 4 + peer_of(g, k))
        send_plane(part, z, True)
        send_plane(part, z, False)

    def far_part(part, far, below):
        src = z - far if below else z + far
        spot = plane_piece(part, src)
        remote(spot, spot, rx_far.at[part, src], rx_far.at[part, src], partner).wait_recv()
        send_plane(part, src, below)

    def far_parts(part):
        for far in range(1, nz):
            for below in (True, False):
                @pl.when((z >= far) if below else (z + far < nz))
                def _():
                    far_part(part, far, below)

    def start_weights(kind, l):
        own_weight(kind, l).start()
        for k in (1, 2, 3):
            give_weight(kind, l, k).start()

    def rows_of(q):
        return pl.ds(HALO + q * own, own)

    halo_here = xt.at[c, pl.ds(0, HALO), :]
    tail = tok.at[pl.ds(own - HALO, HALO), :]
    halo_up = remote(tail, halo_here, halo_tx.at[0], halo.at[0], (sp + 4, c))
    halo_peer = {k: remote(halo_here, halo_here, halo_tx.at[k], halo.at[0], peer(k)) for k in (1, 2, 3)}
    halo_part = remote(halo_here, halo_here, halo_tx.at[4], halo.at[1], partner)

    own_tile = pltpu.make_async_copy(doc_tile, tiles.at[g], tile_rx.at[g])
    own_tile.start()
    tile_sent = [remote(doc_tile, tiles.at[g], tile_tx.at[k], tile_rx.at[g], peer(k)) for k in (1, 2, 3)]
    tile_up = remote(doc_tile, tiles.at[4], tile_tx.at[0], tile_rx.at[4], (sp + 4, c))
    tile_on = [remote(tiles.at[4], tiles.at[4], tile_tx.at[3 + k], tile_rx.at[4], peer(k)) for k in (1, 2, 3)]
    for copy in tile_sent:
        copy.start()

    @pl.when((z < nz - 1) & (g == 3))
    def _():
        halo_up.start()
        tile_up.start()

    for up in (True, False):
        send_relay("in", 0, sp, up, given("in", 0, g))
    start_weights("in", 0)
    start_weights("mix", 0)
    tok_here = pltpu.make_async_copy(tok, xt.at[c, rows_of(g), :], tok_rx.at[0])
    tok_here.start()
    tok_sent = [remote(tok, xt.at[c, rows_of(g), :], tok_ptx.at[0], tok_prx.at[0], partner)]
    for k in (1, 2):
        tok_sent.append(
            remote(tok, xt.at[c, rows_of(g), :], tok_tx.at[k], tok_rx.at[k], peer(k))
        )
    for copy in tok_sent:
        copy.start()

    @pl.when(z == 0)
    def _():
        xt[:, 0:HALO, :] = jnp.zeros((2, HALO, xt.shape[2]), xt.dtype)

    docs[0 : 16 + HALO, :] = jnp.zeros((16 + HALO, 128), jnp.float32)
    proj[0:16, :] = jnp.zeros((16, width), proj.dtype)

    def spread(block, rx, tx, prx, ptx, sent):
        for k in (1, 2):
            spot = block(c, peer_of(g, k))
            remote(spot, spot, rx.at[k], rx.at[k], partner).wait_recv()
        for k in (1, 2):
            part = half_of(block(c, peer_of(g, k)), k)
            copy = remote(part, part, tx.at[2 + k], rx.at[2 + k], peer(3 - k))
            copy.start()
            sent.append(copy)
        for k in (1, 2):
            spot = block(c, peer_of(g, k))
            copy = remote(spot, spot, ptx.at[k], prx.at[k], partner)
            copy.start()
            sent.append(copy)

    def spread_end(block, rx, prx, ptx, sent):
        spot = block(c, peer_of(g, 3))
        for k in (1, 2):
            part = half_of(spot, k)
            remote(part, part, rx.at[2 + k], rx.at[2 + k], partner).wait_recv()
        copy = remote(spot, spot, ptx.at[3], prx.at[3], partner)
        copy.start()
        sent.append(copy)

    def from_partner(block, prx, k):
        spot = block(1 - c, peer_of(g, k))
        remote(spot, spot, prx.at[k], prx.at[k], partner).wait_recv()

    def half_of(spot, k):
        n = spot.shape[0] // 2
        return spot.at[pl.ds((k - 1) * n, n), :]

    def tok_block(side, q):
        return xt.at[side, rows_of(q), :]

    step = 16
    tile = total // 2
    chunk = 32

    def normalize_rows(l, load, start, count):
        def body(i, carry):
            r = pl.ds(pl.multiple_of(start + i * step, step), step)
            squares = jnp.zeros((step, 128), jnp.float32)
            for j in range(8):
                v = load(j, r).astype(jnp.float32)
                v = v * v
                for q in range(width // 128):
                    squares = squares + v[:, q * 128 : (q + 1) * 128]
            mean = jnp.sum(squares, axis=-1, keepdims=True) * (1.0 / (8 * width))
            factor = lax.rsqrt(mean + epsilon)
            for j in range(8):
                v = load(j, r).astype(jnp.float32) * factor
                normed[r, j * width : (j + 1) * width] = (
                    v * gain[l : l + 1, j * width : (j + 1) * width]
                ).astype(jnp.bfloat16)
            return carry

        lax.fori_loop(0, count // step, body, 0, unroll=2)

    def load_tokens(j, r):
        h = j // 4
        return xt[h, r, (j % 4) * width : (j % 4 + 1) * width]

    def load_acts(j, r):
        return acts[j, r, :]

    def add_plane(l, src, first=False):
        ks = pl.ds(pl.multiple_of(src * 4 * k_in, 4 * k_in), 4 * k_in)
        for m in range(2):
            r = slice(m * tile, (m + 1) * tile)
            y = jnp.dot(normed[r, ks], w_in[l, ks, :], preferred_element_type=jnp.float32)
            acc[r, :] = y if first else acc[r, :] + y

    def add_last(l):
        @pl.when((z == 0) | (z == nz - 1))
        def _():
            src = nz - 1 - z
            ks = pl.ds(pl.multiple_of(src * 4 * k_in, 4 * k_in), 4 * k_in)
            for m in range(2):
                r = slice(m * tile, (m + 1) * tile)
                y = jnp.dot(normed[r, ks], w_in[l, ks, :], preferred_element_type=jnp.float32)
                proj[16 + m * tile : 16 + (m + 1) * tile, :] = (acc[r, :] + y).astype(jnp.bfloat16)

        @pl.when((z > 0) & (z < nz - 1))
        def _():
            store_proj()

    def add_far(l, far):
        @pl.when(z >= far)
        def _():
            add_plane(l, z - far)

        @pl.when(z + far < nz)
        def _():
            add_plane(l, z + far)

    def store_proj():
        proj[16 : 16 + total, :] = acc[...].astype(jnp.bfloat16)

    split = total // 2 // chunk * chunk + chunk
    spans = ((0, split), (split, total - split))

    def pool(flags, first, count):
        def body(i, carry):
            base = pl.multiple_of(first + i * chunk, chunk)
            ext = pl.ds(base, chunk + 16)
            d = docs[ext, :]
            same = []
            tally = jnp.ones_like(d)
            for j in range(4):
                ok = jnp.where(pltpu.roll(d, 2**j, 0) == d, flags[j], 0.0)
                same.append(ok)
                tally = tally + ok * pltpu.roll(tally, 2**j, 0)
            share = 1.0 / tally
            for q in range(width // 128):
                cols = slice(q * 128, (q + 1) * 128)
                p = proj[ext, cols].astype(jnp.float32)
                total_sum = p
                for j in range(4):
                    total_sum = total_sum + same[j] * pltpu.roll(total_sum, 2**j, 0)
                v = total_sum * share - p
                pooled[c, pl.ds(base, chunk), cols] = v[16:, :].astype(jnp.bfloat16)
            return carry

        lax.fori_loop(0, count // chunk, body, 0)

    flags = [jnp.where(g >= j, jnp.float32(1.0), jnp.float32(0.0)) for j in range(4)]

    def swap_pooled(l, h):
        here = pooled.at[c, pl.ds(*spans[h]), :]
        return remote(here, here, pool_sem.at[l, h], pool_sem.at[l, 2 + h], partner)

    def pooled_arrived(l, h):
        there = pooled.at[1 - c, pl.ds(*spans[h]), :]
        remote(there, there, pool_sem.at[l, 2 + h], pool_sem.at[l, 2 + h], partner).wait_recv()

    def pool_and_swap(l):
        for h in range(2):
            pool(flags, *spans[h])
            swap_pooled(l, h).start()

    def mix(part, spans, store):
        l, cols = columns("mix", part, 0)
        first = (g + 4 * c) * width + cols.start
        for r in spans:
            y = jnp.dot(
                pooled[0, r, :], w_mix[l, 0:width, cols], preferred_element_type=jnp.float32
            )
            y = y + jnp.dot(
                pooled[1, r, :], w_mix[l, width : 2 * width, cols],
                preferred_element_type=jnp.float32,
            )
            store(r, cols, (y * scale[l : l + 1, pl.ds(pl.multiple_of(first, 128), cols.size)]).astype(jnp.bfloat16))

    def normalize_block(k):
        start = pl.multiple_of(HALO + peer_of(g, k) * own, 16)
        normalize_rows(0, load_tokens, start, own)

    pump_plane("in", 0)
    pump_plane("mix", 0)

    @pl.when((z > 0) & (g == 3))
    def _():
        remote(halo_here, halo_here, halo.at[0], halo.at[0], partner).wait_recv()
        halo_part.start()
        for k in (1, 2, 3):
            halo_peer[k].start()
        remote(tiles.at[4], tiles.at[4], tile_rx.at[4], tile_rx.at[4], partner).wait_recv()
        for copy in tile_on:
            copy.start()

    pump_far("in", 0, 1)
    pump_far("mix", 0, 1)
    tok_here.wait()
    from_partner(tok_block, tok_prx, 0)
    normalize_block(0)
    for far in range(2, nz - 1):
        pump_far("in", 0, far)
        pump_far("mix", 0, far)
    spread(tok_block, tok_rx, tok_tx, tok_prx, tok_ptx, tok_sent)
    start_weights("in", 1)
    for part in LAST_PARTS:
        start_weights("mix", part)

    @pl.when((z > 0) & (g != 3))
    def _():
        remote(halo_here, halo_here, halo.at[0], halo.at[0], partner).wait_recv()
        halo_part.start()
        remote(tiles.at[4], tiles.at[4], tile_rx.at[4], tile_rx.at[4], partner).wait_recv()

    for k in (1, 2):
        from_partner(tok_block, tok_prx, k)
        normalize_block(k)

    @pl.when(z > 0)
    def _():
        spot = xt.at[1 - c, pl.ds(0, HALO), :]
        remote(spot, spot, halo.at[1], halo.at[1], partner).wait_recv()

    normalize_rows(0, load_tokens, 0, HALO)
    spread_end(tok_block, tok_rx, tok_prx, tok_ptx, tok_sent)
    from_partner(tok_block, tok_prx, 3)
    normalize_block(3)
    own_tile.wait()
    for k in (1, 2, 3):
        spot = tiles.at[peer_of(g, k)]
        remote(spot, spot, tile_rx.at[peer_of(g, k)], tile_rx.at[peer_of(g, k)], partner).wait_recv()

    def doc_rows(q, lanes):
        return jnp.broadcast_to(tiles[q, lanes : lanes + 1, :], (128, 128)).T

    for q in range(4):
        for first in range(0, own, 128):
            count = min(128, own - first)
            start = 16 + HALO + q * own + first
            docs[start : start + count, :] = doc_rows(q, first // 128)[:count]

    @pl.when(z > 0)
    def _():
        lead = (own - HALO) % 128
        docs[16 : 16 + HALO, :] = doc_rows(4, (own - HALO) // 128)[lead : lead + HALO]

    own_weight("in", 0).wait()
    add_plane(0, z, True)
    for far in range(1, nz - 1):
        add_far(0, far)
    pump_far("in", 0, nz - 1)
    add_last(0)
    pump_plane("in", 1)
    pool_and_swap(0)
    pump_far("mix", 0, nz - 1)
    inside = (z > 0) & (z < nz - 1)

    @pl.when(jnp.logical_not(inside))
    def _():
        for part in LAST_PARTS:
            pump_own_part(part)

    for h in range(2):
        pooled_arrived(0, h)
    mine = g + 4 * c

    def store_acts(r, cols, v):
        acts[mine, r, cols] = v

    mix(0, [slice(m * tile, (m + 1) * tile) for m in range(2)], store_acts)
    here = acts.at[mine]
    act_sent = [remote(here, here, act_ptx.at[0], act_prx.at[0], partner)]
    for k in (1, 2):
        act_sent.append(remote(here, here, act_tx.at[k], act_rx.at[k], peer(k)))
    for copy in act_sent[1:] + act_sent[:1]:
        copy.start()

    def act_block(side, q):
        return acts.at[q + 4 * side]

    @pl.when(inside)
    def _():
        pump_far("in", 1, 1)
        for far in range(2, nz - 1):
            pump_far("in", 1, far, range(2))

    spread(act_block, act_rx, act_tx, act_prx, act_ptx, act_sent)

    @pl.when(inside)
    def _():
        for far in range(2, nz - 1):
            pump_far("in", 1, far, range(2, 4))

    spread_end(act_block, act_rx, act_prx, act_ptx, act_sent)

    @pl.when(inside)
    def _():
        for part in LAST_PARTS:
            pump_own_part(part)

    for k in range(4):
        from_partner(act_block, act_prx, k)
    normalize_rows(1, load_acts, 0, total)
    @pl.when(jnp.logical_not(inside))
    def _():
        for far in range(1, nz - 1):
            pump_far("in", 1, far)

    add_plane(1, z, True)
    for far in range(1, nz - 1):
        add_far(1, far)

    @pl.when((z == 0) | (z == nz - 1))
    def _():
        for k in range(4):
            arrived("in", 1, (nz - 1 - z) * 4 + peer_of(g, k))

    add_last(1)
    for h in range(2):
        swap_pooled(0, h).wait_send()
    pool_and_swap(1)
    @pl.when(inside)
    def _():
        for part in LAST_PARTS:
            far_parts(part)

    def store_last(r, cols, v):
        last[r, cols] = v

    def out_copy(part, k):
        _, place = columns("mix", part, g)
        _, cols = columns("mix", part, 0)
        src = last.at[rows_of(peer_of(g, k)), cols]
        dst = out.at[:, place]
        if k == 0:
            return pltpu.make_async_copy(src, dst, out_rx.at[part, 0])
        return remote(src, dst, out_tx.at[part, k], out_rx.at[part, k], peer(k))

    for part in LAST_PARTS:
        @pl.when(jnp.logical_not(inside))
        def _():
            far_parts(part)

        if part == 1:
            for h in range(2):
                pooled_arrived(1, h)
        for k in (3, 1, 2, 0):
            start = pl.multiple_of(HALO + peer_of(g, k) * own, 16)
            mix(part, [pl.ds(start, own)], store_last)
            out_copy(part, k).start()

    for h in range(2):
        swap_pooled(1, h).wait_send()
    for kind in ("in", "mix"):
        for l in range(2 if kind == "in" else len(PARTS)):
            for k in (1, 2, 3):
                give_weight(kind, l, k).wait_send()
            if kind == "mix" and l:
                continue
            for src in range(nz):
                for k in range(4):
                    s = src * 4 + k

                    @pl.when((z >= src) & (z < nz - 1))
                    def _():
                        relay(kind, l, s, True).wait_send()

                    @pl.when((z <= src) & (z > 0))
                    def _():
                        relay(kind, l, s, False).wait_send()

    for part in LAST_PARTS:
        for src in range(nz):
            @pl.when((z >= src) & (z < nz - 1))
            def _():
                plane_relay(part, src, True).wait_send()

            @pl.when((z <= src) & (z > 0))
            def _():
                plane_relay(part, src, False).wait_send()

    for copy in tile_sent:
        copy.wait_send()

    @pl.when((z < nz - 1) & (g == 3))
    def _():
        halo_up.wait_send()
        tile_up.wait_send()

    @pl.when(z > 0)
    def _():
        halo_part.wait_send()

        @pl.when(g == 3)
        def _():
            for k in (1, 2, 3):
                halo_peer[k].wait_send()
            for copy in tile_on:
                copy.wait_send()

    for copy in tok_sent + act_sent:
        copy.wait_send()
    for part in LAST_PARTS:
        for k in (1, 2, 3):
            _, place = columns("mix", part, peer_of(g, k))
            _, cols = columns("mix", part, 0)
            remote(
                last.at[rows_of(peer_of(g, k)), cols], out.at[:, place],
                out_tx.at[part, k], out_rx.at[part, k], peer(k),
            ).wait()
        out_copy(part, 0).wait()


def fused_shards(tokens, doc_ids, norm_gain, in_proj, mix_proj, out_scale):
    own, local_width = tokens.shape
    width = local_width // 4
    nsp = lax.axis_size("sp")
    nz = nsp // 4
    total = HALO + 4 * own
    numbers = (doc_ids + 1).astype(jnp.float32)
    doc_tile = jnp.pad(numbers, (0, 8 * 128 - own)).reshape(8, 128)
    any_spec = pl.BlockSpec(memory_space=pl.ANY)
    vmem_spec = pl.BlockSpec(memory_space=pltpu.VMEM)
    bf16, f32 = jnp.bfloat16, jnp.float32
    dma = pltpu.SemaphoreType.DMA
    scratch = [
        pltpu.VMEM((2, total, local_width), bf16),
        pltpu.VMEM((total, 8 * width), bf16),
        pltpu.VMEM((8, total, width), bf16),
        pltpu.VMEM((2, 8 * width, width), bf16),
        pltpu.VMEM((2, 2 * width, width), bf16),
        pltpu.VMEM((total, width), f32),
        pltpu.VMEM((16 + total, width), bf16),
        pltpu.VMEM((16 + total, 128), f32),
        pltpu.VMEM((2, total, width), bf16),
        pltpu.VMEM((total, width), bf16),
    ]
    parts = len(PARTS)
    scratch += [dma((n, nsp)) for _ in range(3) for n in (2, parts)]
    scratch += [dma((2, 4)), dma((parts, 4)), dma((parts, 4))]
    scratch += [pltpu.VMEM((5, 8, 128), f32), dma((5,)), dma((7,))]
    scratch += [dma((5,)) for _ in range(4)] + [dma((2,)), dma((5,))]
    scratch += [dma((5,)) for _ in range(4)] + [dma((2, 4)), dma((parts, 4)), dma((parts, 4))]
    return pl.pallas_call(
        functools.partial(fused_kernel, nz, own),
        out_shape=jax.ShapeDtypeStruct((own, local_width), bf16),
        in_specs=[any_spec, vmem_spec, any_spec, any_spec, vmem_spec, vmem_spec],
        out_specs=any_spec,
        scratch_shapes=scratch,
        compiler_params=pltpu.CompilerParams(
            collective_id=0, has_side_effects=True, vmem_limit_bytes=60 * 1024 * 1024
        ),
    )(tokens, doc_tile, in_proj, mix_proj, norm_gain, out_scale)


def solution(mesh):
    placed = (P("sp", "tp"), P("sp"), P(), P(None, "sp", "tp"), P(None, "sp", "tp"), P())
    body = fused_shards if mesh.shape["tp"] == 2 and mesh.shape["sp"] == 16 else shards
    return jax.shard_map(
        body, mesh=mesh, in_specs=placed, out_specs=P("sp", "tp"), check_vma=False
    )
```
